32 devices in a mesh: sp: 8 (over z, x), tp: 4 (over y, core).
Axes of the slice: x: 2, y: 2, z: 4, core: 2. Of those that a mesh axis runs over, the one named last changes fastest.
Arguments:
- tokens: bfloat16 [1024, 2048], P('sp'), may hold values from -6 to 6
- query_narrow: bfloat16 [1024, 2048], P('sp', 'tp'), may hold values from -20 to 20
- key_narrow: bfloat16 [1024, 2048], P('sp', 'tp'), may hold values from -20 to 20
- value_narrow: bfloat16 [1024, 2048], P('sp', 'tp'), may hold values from -6 to 6
- query_broad: bfloat16 [1024, 4096], P('sp', 'tp'), may hold values from -20 to 20
- key_broad: bfloat16 [1024, 4096], P('sp', 'tp'), may hold values from -20 to 20
- value_broad: bfloat16 [1024, 2048], P('sp', 'tp'), may hold values from -6 to 6
- mix_lambda: float32 [2, 16], P(None, 'tp'), may hold values from 0.3 to 0.8
- head_gain: float32 [2, 128], replicated, may hold values from 0.1 to 1.9
- proj_narrow: bfloat16 [2048, 2048], P('tp'), may hold values from -0.09375 to 0.09375
- proj_broad: bfloat16 [2048, 2048], P('tp'), may hold values from -0.09375 to 0.09375
- gain_one: float32 [2048], replicated, may hold values from 0.1 to 1.9
- gain_two: float32 [2048], replicated, may hold values from 0.1 to 1.9
- expert_ids: int32 [1024, 2], P('sp'), may hold values from 0 to 31, all different within a row; in each aligned block of 128 rows (0 to 127, 128 to 255, ...) at most 16 rows name the same one
- expert_gates: float32 [1024, 2], P('sp'), may hold values from 0.1 to 0.9
- gate_weight: bfloat16 [32, 2048, 4096], P('sp', None, 'tp'), may hold values from -0.125 to 0.125
- up_weight: bfloat16 [32, 2048, 4096], P('sp', None, 'tp'), may hold values from -0.125 to 0.125
- down_weight: bfloat16 [32, 4096, 2048], P('sp', 'tp'), may hold values from -0.09375 to 0.09375
Outputs:
- result: bfloat16 [1024, 2048], P('sp')
The draws below stay inside these ranges and needn't reach their ends.
Inputs may be any that keep to these rules, and one draw needn't show every extreme that they name: `expert_ids`: the 2 experts of a token differ. Among the tokens of one index of sp (aligned blocks of 128 tokens) no expert is named by more than 16 tokens, and in some blocks one expert is named by exactly 16.
All inputs are finite; a program needn't handle non-finite values.
Results may differ from the reference program's by a relative error of at most 0.015.
Values may be sent and summed in bfloat16 or wider, within the bound.
A program may use at most 128 MiB of HBM per device.

```python
import math
import jax
import jax.numpy as jnp
import numpy as np
from jax import lax

D = 2048
HEADS = 16
QK_NARROW = 64
QK_BROAD = 128
V = 128
EXPERTS = 32
FF_EXP = 4096
TOP = 2
CAP = 16
TOK_DEV = 128
TOKENS = 1024
N_SP = 8
N_TP = 4


def draw_queries(key, key_width, salt):
    base = jax.random.normal(jax.random.fold_in(key, salt), (TOKENS, HEADS, 2, key_width), jnp.float32)
    base = jnp.clip(base * 1.35, -8.0, 8.0)
    return base.reshape(TOKENS, HEADS * 2 * key_width).astype(jnp.bfloat16)


def draw_keys(key, key_width, salt):
    base = jax.random.normal(jax.random.fold_in(key, salt), (TOKENS, HEADS, 2, key_width), jnp.float32)
    base = jnp.clip(base * 1.35, -8.0, 8.0)
    return base.reshape(TOKENS, HEADS * 2 * key_width).astype(jnp.bfloat16)


def draw_query_narrow(key, part):
    return draw_queries(key, QK_NARROW, 31)


def draw_key_narrow(key, part):
    return draw_keys(key, QK_NARROW, 32)


def draw_query_broad(key, part):
    return draw_queries(key, QK_BROAD, 33)


def draw_key_broad(key, part):
    return draw_keys(key, QK_BROAD, 34)


def block_scale(own_key, shape, cuts, least, top_value):
    factor_of, own = 1.0, jax.random.fold_in(own_key, 6)
    for axis_at, blocks in cuts:
        steps = jnp.exp(jax.random.uniform(jax.random.fold_in(own, axis_at), (blocks,), jnp.float32, least / len(cuts), top_value / len(cuts)))
        factor_of = factor_of * jnp.repeat(steps, shape[axis_at] // blocks).reshape([-1 if axis == axis_at else 1 for axis in range(len(shape))])
    return factor_of


def shared_out(own_key, own, number, rows, count, top, most, lean):
    sequence = jax.random.permutation(own_key, count)
    heavy_load, common = portions_of(count, rows * top, most, lean, True), portions_of(count, rows * top, most, lean, False)
    places = jnp.arange(count)

    def named(lengths, rotation):
        used = int((lengths > 0).sum())
        fixed = max(1, used // 4)
        moved = fixed + (places - fixed + rotation * (used - fixed)) % max(1, count - fixed)
        return jnp.zeros((count,), jnp.int32).at[sequence[jnp.where(places < fixed, places, moved)]].set(jnp.asarray(lengths, jnp.int32))

    lengths = jnp.where(number % 4 == 0, named(heavy_load, number // 4), named(common, number - number // 4 - 1))
    mixed = jax.random.permutation(jax.random.fold_in(own, 3), count)
    donor, taker = mixed[0:count // 2 * 2:2], mixed[1:count // 2 * 2:2]
    margin = jnp.minimum(lengths[donor] - 1, most - lengths[taker]) // 2
    margin = jnp.where((donor == sequence[0]) | (taker == sequence[0]) | (lengths[taker] == 0), 0, jnp.maximum(margin, 0))
    moved = jax.random.randint(jax.random.fold_in(own, 4), (count // 2,), 0, 1 << 20) % (margin + 1)
    lengths = lengths.at[donor].add(-moved).at[taker].add(moved)
    items = jnp.searchsorted(jnp.cumsum(lengths), jnp.arange(rows * top), side="right").astype(jnp.int32)
    listing = items.reshape(top, rows).T
    listing = listing[jax.random.permutation(jax.random.fold_in(own, 1), rows)]
    rotation = jax.random.randint(jax.random.fold_in(own, 2), (rows, 1), 0, top)
    return jnp.take_along_axis(listing, (jnp.arange(top)[None, :] + rotation) % top, axis=1)


def portions_of(amount, total, most, lean, full):
    weights = [(1 << 20) // math.isqrt(standing ** lean) + 1 for standing in range(1, amount + 1)]
    largest = most if full else min(most, max(-(-total // amount), total * weights[0] // sum(weights)))
    least = 1 if total - largest >= amount - 1 else 0
    given, spare = [largest] + [least] * (amount - 1), total - largest - least * (amount - 1)
    while spare > 0:
        movable = [i for i in range(1, amount) if given[i] < largest] or [i for i in range(1, amount) if given[i] < most]
        whole, budget = sum([weights[i] for i in movable]), spare
        for i in movable:
            extra = min(most - given[i], max(1, budget * weights[i] // whole), spare)
            given[i] = given[i] + extra
            spare = spare - extra
    return np.array(given)


def noise(own_key, dims, deviation, reach, split=(), kind=jnp.bfloat16):
    level = block_scale(own_key, dims, split, -0.22, 0.18) if split else 1.0
    values = jax.random.normal(own_key, dims, jnp.float32) * deviation * level
    return jnp.minimum(jnp.maximum(values, -reach), reach).astype(kind)


def setup_inputs(seed: int = 0) -> dict:
    arg_keys = jax.random.split(jax.random.key(seed), 19)
    tokens = noise(arg_keys[0], (TOKENS, D), 1.0, 6.0, ((0, 8),))
    query_narrow = draw_query_narrow(jax.random.fold_in(arg_keys[18], 71), 0)
    key_narrow = draw_key_narrow(jax.random.fold_in(arg_keys[18], 71), 0)
    value_narrow = noise(arg_keys[3], (TOKENS, HEADS * V), 1.0, 6.0, ((0, 8), (1, 4)))
    query_broad = draw_query_broad(jax.random.fold_in(arg_keys[18], 71), 0)
    key_broad = draw_key_broad(jax.random.fold_in(arg_keys[18], 71), 0)
    value_broad = noise(arg_keys[6], (TOKENS, HEADS * V), 1.0, 6.0, ((0, 8), (1, 4)))
    mix_lambda = jnp.clip(0.3 + 0.5 * jax.random.uniform(arg_keys[7], (2, HEADS), jnp.float32) ** block_scale(arg_keys[7], (2, HEADS), ((1, 4),), -0.2, 0.2), 0.3, 0.8)
    head_gain = jnp.clip(1.0 + 0.18 * jax.random.normal(arg_keys[8], (2, V), jnp.float32), 0.1, 1.9)
    proj_narrow = noise(arg_keys[9], (HEADS * V, D), (2 * HEADS * V) ** -0.5, 0.09375, ((0, 4),))
    proj_broad = noise(arg_keys[10], (HEADS * V, D), (2 * HEADS * V) ** -0.5, 0.09375, ((0, 4),))
    gain_one = jnp.clip(1.0 + 0.18 * jax.random.normal(arg_keys[11], (D,), jnp.float32), 0.1, 1.9)
    gain_two = jnp.clip(1.0 + 0.18 * jax.random.normal(arg_keys[12], (D,), jnp.float32), 0.1, 1.9)
    expert_ids_keys = jax.random.split(jax.random.fold_in(arg_keys[13], 1), TOKENS // TOK_DEV)
    expert_ids_turns = jax.random.permutation(jax.random.fold_in(arg_keys[13], 3), TOKENS // TOK_DEV)
    expert_ids = jax.vmap(lambda own, number: shared_out(jax.random.fold_in(arg_keys[13], 2), own, number, TOK_DEV, EXPERTS, TOP, CAP, 2))(expert_ids_keys, expert_ids_turns).reshape((TOKENS, TOP))
    expert_gates = jnp.clip(0.1 + 0.79999997 * jax.random.uniform(arg_keys[14], (TOKENS, TOP), jnp.float32) ** block_scale(arg_keys[14], (TOKENS, TOP), ((0, 8),), -0.2, 0.2), 0.1, 0.9)
    gate_weight = noise(arg_keys[15], (EXPERTS, D, FF_EXP), D ** -0.5, 0.125, ((0, 8), (2, 4)))
    up_weight = noise(arg_keys[16], (EXPERTS, D, FF_EXP), D ** -0.5, 0.125, ((0, 8), (2, 4)))
    down_weight = noise(arg_keys[17], (EXPERTS, FF_EXP, D), FF_EXP ** -0.5, 0.09375, ((0, 8), (1, 4)))
    return dict(tokens=tokens, query_narrow=query_narrow, key_narrow=key_narrow, value_narrow=value_narrow, query_broad=query_broad, key_broad=key_broad, value_broad=value_broad, mix_lambda=mix_lambda, head_gain=head_gain, proj_narrow=proj_narrow, proj_broad=proj_broad, gain_one=gain_one, gain_two=gain_two, expert_ids=expert_ids, expert_gates=expert_gates, gate_weight=gate_weight, up_weight=up_weight, down_weight=down_weight)


deep_alpha = 8.0 ** 0.25
norm_eps = 1e-05

def layer_scale(inputs, gains):
    center = lax.optimization_barrier(jnp.mean(inputs, -1, keepdims=True))
    spread = lax.optimization_barrier(jnp.mean(jnp.square(inputs - center), -1, keepdims=True))
    return (inputs - center) * lax.rsqrt(spread + norm_eps) * gains

def group_heads(queries, key_rows, values, mixing, gains, key_width):
    count = queries.shape[0]
    stacked_q = jnp.moveaxis(queries.reshape(count, HEADS, 2, key_width), 1, 0)
    stacked_k = jnp.moveaxis(key_rows.reshape(count, HEADS, 2, key_width), 1, 0)
    stacked_v = jnp.moveaxis(values.reshape(count, HEADS, V), 1, 0)
    factor = key_width ** (-0.5)

    def one_head(members):
        head_q, head_k, head_v, weight = members
        scores = jnp.einsum('qmd,kmd->mqk', head_q.astype(jnp.float32), head_k.astype(jnp.float32)) * factor
        highest = lax.optimization_barrier(jnp.max(scores, -1, keepdims=True))
        exponent = jnp.exp(scores - highest)
        totals = lax.optimization_barrier(jnp.sum(exponent, -1))
        probs = lax.optimization_barrier(exponent.astype(jnp.bfloat16))
        numer = jnp.einsum('mqk,kv->mqv', probs.astype(jnp.float32), head_v.astype(jnp.float32))
        diff = numer[0] / totals[0][:, None] - weight * numer[1] / totals[1][:, None]
        normed = diff * lax.rsqrt(lax.optimization_barrier(jnp.mean(diff * diff, -1, keepdims=True)) + norm_eps) * gains
        return normed.astype(jnp.bfloat16)
    output = lax.map(one_head, (stacked_q, stacked_k, stacked_v, mixing))
    return jnp.moveaxis(output, 0, 1).reshape(count, HEADS * V)

def attention_sum(heads_first, heads_second, proj_narrow, proj_broad):
    count = heads_first.shape[0]
    block_width = HEADS // N_TP * V
    first_blocks = jnp.moveaxis(heads_first.reshape(count, N_TP, block_width), 1, 0)
    second_blocks = jnp.moveaxis(heads_second.reshape(count, N_TP, block_width), 1, 0)
    first_weights = proj_narrow.reshape(N_TP, block_width, D)
    second_weights = proj_broad.reshape(N_TP, block_width, D)

    def add_block(running, members):
        part_one, part_two, weight_one, weight_two = members
        partial_value = jnp.dot(part_one, weight_one, preferred_element_type=jnp.float32)
        partial_value = partial_value + jnp.dot(part_two, weight_two, preferred_element_type=jnp.float32)
        rounded = lax.optimization_barrier(partial_value.astype(jnp.bfloat16))
        return (running + rounded.astype(jnp.float32), None)
    running, _ = lax.scan(add_block, jnp.zeros((count, D), jnp.float32), (first_blocks, second_blocks, first_weights, second_weights))
    return running

def one_expert(members):
    expert_rows, gate_part, up_part, down_part = members
    activated = (jax.nn.silu(jnp.dot(expert_rows, gate_part, preferred_element_type=jnp.float32)) * jnp.dot(expert_rows, up_part, preferred_element_type=jnp.float32)).astype(jnp.bfloat16)
    block_width = FF_EXP // N_TP
    act_blocks = jnp.moveaxis(activated.reshape(expert_rows.shape[0], N_TP, block_width), 1, 0)
    down_blocks = down_part.reshape(N_TP, block_width, D)

    def add_block(running, operands):
        product = jnp.dot(operands[0], operands[1], preferred_element_type=jnp.float32)
        rounded = lax.optimization_barrier(product.astype(jnp.bfloat16))
        return (running + rounded.astype(jnp.float32), None)
    running, _ = lax.scan(add_block, jnp.zeros((expert_rows.shape[0], D), jnp.float32), (act_blocks, down_blocks))
    return running.astype(jnp.bfloat16)

def reference(tokens, query_narrow, key_narrow, value_narrow, query_broad, key_broad, value_broad, mix_lambda, head_gain, proj_narrow, proj_broad, gain_one, gain_two, expert_ids, expert_gates, gate_weight, up_weight, down_weight):
    heads_first = group_heads(query_narrow, key_narrow, value_narrow, mix_lambda[0], head_gain[0], QK_NARROW)
    heads_second = group_heads(query_broad, key_broad, value_broad, mix_lambda[1], head_gain[1], QK_BROAD)
    attn = attention_sum(heads_first, heads_second, proj_narrow, proj_broad)
    mixed_rows = layer_scale(deep_alpha * tokens.astype(jnp.float32) + attn, gain_one).astype(jnp.bfloat16)
    chosen = expert_ids.reshape(N_SP, TOK_DEV * TOP).astype(jnp.int32)
    onehot = (chosen[:, :, None] == jnp.arange(EXPERTS, dtype=jnp.int32)[None, None, :]).astype(jnp.int32)
    before = jnp.cumsum(onehot, axis=1, dtype=jnp.int32) - onehot
    slot_index = lax.optimization_barrier(jnp.sum(before * onehot, axis=-1, dtype=jnp.int32))
    block_index = jnp.arange(N_SP, dtype=jnp.int32)[:, None]
    position = ((chosen * N_SP + block_index) * CAP + slot_index).reshape(-1).astype(jnp.int32)
    repeated = jnp.repeat(mixed_rows, TOP, axis=0)
    buffer = jnp.zeros((EXPERTS * N_SP * CAP, D), jnp.bfloat16).at[position].set(repeated)
    buffer = buffer.reshape(EXPERTS, N_SP * CAP, D)
    outputs = lax.map(one_expert, (buffer, gate_weight, up_weight, down_weight))
    picked = outputs.reshape(EXPERTS * N_SP * CAP, D)[position].reshape(N_SP * TOK_DEV, TOP, D)
    routed = lax.optimization_barrier(jnp.sum(expert_gates[:, :, None] * picked.astype(jnp.float32), axis=1))
    return layer_scale(deep_alpha * mixed_rows.astype(jnp.float32) + routed, gain_two).astype(jnp.bfloat16)
```

```python
import functools

import jax
import jax.numpy as jnp
from jax import lax
from jax.experimental import pallas as pl
from jax.experimental.pallas import tpu as pltpu
from jax.sharding import PartitionSpec as P

QK_NARROW = 64
QK_BROAD = 128
V = 128
TOP = 2
CAP = 16


deep_alpha = 8.0**0.25
norm_eps = 1e-05


def layer_scale(inputs, gains):
    center = jnp.mean(inputs, -1, keepdims=True)
    spread = jnp.mean(jnp.square(inputs - center), -1, keepdims=True)
    return (inputs - center) * lax.rsqrt(spread + norm_eps) * gains


MESH = pl.DeviceIdType.MESH
LOG2E = 1.4426950408889634


def remote(src, dst, send, recv, axis, index):
    return pltpu.make_async_remote_copy(
        src_ref=src,
        dst_ref=dst,
        send_sem=send,
        recv_sem=recv,
        device_id={axis: index},
        device_id_type=MESH,
    )


def greet(n_sp, n_tp, sp, tp):
    barrier = pltpu.get_barrier_semaphore()
    for k in range(1, n_sp):
        pl.semaphore_signal(
            barrier, inc=1, device_id={"sp": lax.rem(sp + k, n_sp)}, device_id_type=MESH
        )
    for k in range(1, n_tp):
        pl.semaphore_signal(
            barrier, inc=1, device_id={"tp": lax.rem(tp + k, n_tp)}, device_id_type=MESH
        )
    pl.semaphore_wait(barrier, n_sp + n_tp - 2)


def lanes(index, width):
    return pl.ds(pl.multiple_of(index * width, width), width)


def expert_kernel(
    n_sp, n_tp, mixed, spread, high, low, gain_two, wg, wu, wd, out,
    gate, up, down, rows_out, rows_in, act, part, part_core, part_far, summed, back, routed,
    loaded, a_send, a_recv, y_send, y_recv, c_send, c_recv,
    d_send, d_recv, s_send, s_recv, b_send, b_recv, g_send, g_recv,
):
    sp, tp = lax.axis_index("sp"), lax.axis_index("tp")
    experts, slots, width = rows_out.shape[1:]
    hidden = act.shape[1]
    filled = n_sp * slots
    pairs = n_tp // 2
    y, c = tp // 2, tp % 2
    other = 2 * y + 1 - c

    def load(e, go):
        for i, (a, b) in enumerate(((wg, gate), (wu, up), (wd, down))):
            copy = pltpu.make_async_copy(a.at[e], b.at[e], loaded.at[i, e])
            copy.start() if go else copy.wait()

    def each(body):
        lax.fori_loop(0, experts, lambda e, _: (body(e), 0)[1], 0)

    each(lambda e: load(e, True))
    greet(n_sp, n_tp, sp, tp)

    mine = lanes(tp, width)
    picked = jnp.dot(spread[...], mixed[:, mine], preferred_element_type=jnp.float32)
    rows_out[...] = picked.astype(jnp.bfloat16).reshape(rows_out.shape)

    def dispatch(e, k):
        to = lax.rem(sp + k, n_sp)
        return remote(
            rows_out.at[to, e], rows_in.at[tp, e, sp], a_send.at[e, k], a_recv.at[e, k], "sp", to
        )

    def send_rows(e):
        for k in range(1, n_sp):
            dispatch(e, k).start()
        rows_in[tp, e, sp] = rows_out[sp, e]

    each(send_rows)

    def far(e, k):
        block = rows_in.at[tp, e]
        to = 2 * lax.rem(y + k, pairs) + c
        return remote(block, block, y_send.at[e, k], y_recv.at[e, k], "tp", to)

    def far_slot(k):
        return 2 * lax.rem(y + pairs - k, pairs) + c

    def across(e, k):
        block = rows_in.at[far_slot(k), e]
        return remote(block, block, c_send.at[e, k], c_recv.at[e, k], "tp", other)

    def pass_on(e):
        for k in range(1, n_sp):
            source = lax.rem(sp + n_sp - k, n_sp)
            block = rows_in.at[tp, e, source]
            remote(block, block, a_send.at[e, k], a_recv.at[e, k], "sp", source).wait_recv()
        for k in range(1, pairs):
            far(e, k).start()
        across(e, 0).start()

    each(pass_on)

    def pass_across(e):
        for k in range(1, pairs):
            block = rows_in.at[far_slot(k), e]
            remote(block, block, y_send.at[e, k], y_recv.at[e, k], "tp", far_slot(k)).wait_recv()
            across(e, k).start()

    def to_core(e, k):
        yy = lax.rem(y + k, pairs)
        return remote(
            part.at[2 * yy + 1 - c, e], part_core.at[k, e], d_send.at[e, k], d_recv.at[e, k],
            "tp", other,
        )

    def to_far(e, k):
        to = 2 * lax.rem(y + k, pairs) + c
        return remote(
            part.at[to, e], part_far.at[k, e], s_send.at[e, k], s_recv.at[e, k], "tp", to
        )

    def give_back(e, k):
        to = lax.rem(sp + k, n_sp)
        return remote(
            summed.at[e, to], back.at[sp, e], b_send.at[e, k], b_recv.at[e, k], "sp", to
        )

    tile = min(256, hidden)

    def compute(e):
        pass_across(e)
        load(e, False)
        for k in range(pairs):
            block = rows_in.at[2 * lax.rem(y + pairs - k, pairs) + 1 - c, e]
            remote(block, block, c_send.at[e, k], c_recv.at[e, k], "tp", other).wait_recv()
        inputs = jnp.concatenate(
            [rows_in[t, e].reshape(filled, width) for t in range(n_tp)], axis=1
        )

        def hidden_tile(j, _):
            cut = lanes(j, tile)
            gated = jnp.dot(inputs, gate[e, :, cut], preferred_element_type=jnp.float32)
            lifted = jnp.dot(inputs, up[e, :, cut], preferred_element_type=jnp.float32)
            act[:, cut] = (gated / (1.0 + jnp.exp(-gated)) * lifted).astype(jnp.bfloat16)
            return 0

        lax.fori_loop(0, hidden // tile, hidden_tile, 0)

        def down_tile(t, _):
            product = jnp.dot(
                act[...], down[e, :, lanes(t, width)], preferred_element_type=jnp.float32
            )
            part[t, e] = product.astype(jnp.bfloat16)
            return 0

        lax.fori_loop(0, n_tp, down_tile, 0)
        for k in range(pairs):
            to_core(e, k).start()

    def core_sum(e, k):
        block = part_core.at[k, e]
        remote(block, block, d_send.at[e, k], d_recv.at[e, k], "tp", other).wait_recv()
        slot = 2 * lax.rem(y + k, pairs) + c
        return part[slot, e].astype(jnp.float32) + part_core[k, e].astype(jnp.float32)

    def reduce_core(e):
        for k in range(1, pairs):
            total = core_sum(e, k)
            part[2 * lax.rem(y + k, pairs) + c, e] = total.astype(jnp.bfloat16)
            to_far(e, k).start()

    def reduce_far(e):
        total = core_sum(e, 0)
        for k in range(1, pairs):
            block = part_far.at[k, e]
            remote(block, block, s_send.at[e, k], s_recv.at[e, k], "tp", far_slot(k)).wait_recv()
            total = total + part_far[k, e].astype(jnp.float32)
        summed[e] = total.astype(jnp.bfloat16).reshape(n_sp, slots, width)
        for k in range(1, n_sp):
            give_back(e, k).start()
        back[sp, e] = summed[e, sp]

    def step(e, _):
        pl.when(e < experts)(lambda: compute(e))
        pl.when((e >= 1) & (e <= experts))(lambda: reduce_core(e - 1))
        pl.when(e >= 2)(lambda: reduce_far(e - 2))
        return 0

    lax.fori_loop(0, experts + 2, step, 0)

    def arrive(e):
        for k in range(1, n_sp):
            source = lax.rem(sp + n_sp - k, n_sp)
            block = back.at[source, e]
            remote(block, block, b_send.at[e, k], b_recv.at[e, k], "sp", source).wait_recv()

    each(arrive)
    returned = back[...].reshape(n_sp * experts * slots, width)
    weighted = jnp.dot(high[...], returned, preferred_element_type=jnp.float32) + jnp.dot(
        low[...], returned, preferred_element_type=jnp.float32
    )
    routed[:, mine] = weighted.astype(jnp.bfloat16)

    def share(k):
        to = lax.rem(tp + k, n_tp)
        block = routed.at[:, mine]
        return remote(block, block, g_send.at[k], g_recv.at[k], "tp", to)

    for k in range(1, n_tp):
        share(k).start()
    for k in range(1, n_tp):
        peer = lax.rem(tp + n_tp - k, n_tp)
        block = routed.at[:, lanes(peer, width)]
        remote(block, block, g_send.at[k], g_recv.at[k], "tp", peer).wait_recv()
    full = deep_alpha * mixed[...].astype(jnp.float32) + routed[...].astype(jnp.float32)
    out[...] = layer_scale(full, gain_two[...]).astype(jnp.bfloat16)

    def sent(e):
        for k in range(1, n_sp):
            dispatch(e, k).wait_send()
            give_back(e, k).wait_send()
        for k in range(pairs):
            across(e, k).wait_send()
            to_core(e, k).wait_send()
        for k in range(1, pairs):
            far(e, k).wait_send()
            to_far(e, k).wait_send()

    each(sent)
    for k in range(1, n_tp):
        share(k).wait_send()


def expert_rows(mixed, spread, high, low, gain_two, wg, wu, wd):
    n_sp, n_tp = lax.axis_size("sp"), lax.axis_size("tp")
    count, model_width = mixed.shape
    experts, hidden = wg.shape[0], wg.shape[2]
    width, pairs, filled = model_width // n_tp, n_tp // 2, n_sp * CAP
    bf16 = jnp.bfloat16
    dma = pltpu.SemaphoreType.DMA
    far = pl.BlockSpec(memory_space=pl.ANY)
    near = pl.BlockSpec(memory_space=pltpu.VMEM)
    vmem = lambda *shape: pltpu.VMEM(shape, bf16)
    return pl.pallas_call(
        functools.partial(expert_kernel, n_sp, n_tp),
        out_shape=jax.ShapeDtypeStruct(mixed.shape, bf16),
        in_specs=[near] * 5 + [far] * 3,
        out_specs=near,
        scratch_shapes=[
            vmem(*wg.shape),
            vmem(*wu.shape),
            vmem(*wd.shape),
            vmem(n_sp, experts, CAP, width),
            vmem(n_tp, experts, n_sp, CAP, width),
            vmem(filled, hidden),
            vmem(n_tp, experts, filled, width),
            vmem(pairs, experts, filled, width),
            vmem(pairs, experts, filled, width),
            vmem(experts, n_sp, CAP, width),
            vmem(n_sp, experts, CAP, width),
            vmem(count, model_width),
            dma((3, experts)),
        ]
        + [dma((experts, n_sp))] * 2
        + [dma((experts, pairs))] * 8
        + [dma((experts, n_sp))] * 2
        + [dma((n_tp,))] * 2,
        compiler_params=pltpu.CompilerParams(
            collective_id=1, has_side_effects=True, vmem_limit_bytes=67043328
        ),
        name="experts",
    )(mixed, spread, high, low, gain_two[None, :], wg, wu, wd)


def flip(index, mask):
    bit = 1
    while bit <= mask:
        if mask & bit:
            index = index + bit - 2 * bit * lax.rem(index // bit, 2)
        bit *= 2
    return index


def route(ids, gates, spread, shares, experts_all):
    count = ids.shape[1]
    expert = lax.broadcasted_iota(jnp.int32, (experts_all, count), 0)
    picks = [(expert == ids[k : k + 1, :]).astype(jnp.float32) for k in range(TOP)]
    taken = functools.reduce(lambda a, b: a + b, picks)
    earlier = lax.broadcasted_iota(jnp.int32, (count, count), 0) < lax.broadcasted_iota(
        jnp.int32, (count, count), 1
    )
    before = jnp.dot(
        taken.astype(jnp.bfloat16),
        earlier.astype(jnp.float32).astype(jnp.bfloat16),
        preferred_element_type=jnp.float32,
    )
    place = lax.broadcasted_iota(jnp.int32, (experts_all * CAP, count), 0).astype(jnp.float32)
    weight = jnp.zeros((experts_all * CAP, count), jnp.float32)
    marked = jnp.zeros((experts_all * CAP, count), jnp.float32)
    for k in range(TOP):
        slot = jnp.sum(before * picks[k], 0, keepdims=True)
        position = ids[k : k + 1, :].astype(jnp.float32) * CAP + slot
        hit = place == position
        weight = weight + jnp.where(hit, gates[k : k + 1, :], 0.0)
        marked = marked + jnp.where(hit, 1.0, 0.0)
    spread[...] = marked.astype(jnp.bfloat16)
    shares[...] = weight.T.astype(jnp.bfloat16)


def layer_kernel(
    n_sp, n_tp, heads, lam_h, ids_h, gates_h, tok_h, qn_h, kn_h, vn_h, qb_h, kb_h, vb_h,
    gains_h, pn_h, pb_h, one_h, two_h, wg, wu, wd, out,
    lam, ids, gates, tok, qn, kn, vn, qb, kb, vb, gains, proj_n, proj_b, gain_one, gain_two,
    gate, up, down, q_all, k_all, v_all, head_out, head_in, early, pc_out, pc_in, py_out, py_in,
    st_out, st_in, mixed, spread, shares, rows_out, rows_in, act, part, part_core, part_far,
    summed, back, z_all,
    local, loaded, send, recv, head_send, head_recv, pc_send, pc_recv, py_send, py_recv,
    st_send, st_recv, a_send, a_recv, y_send, y_recv, c_send, c_recv, d_send, d_recv,
    s_send, s_recv, b_send, b_recv, g_send, g_recv,
):
    sp, tp = lax.axis_index("sp"), lax.axis_index("tp")
    y, c = tp // 2, lax.rem(tp, 2)
    core = 2 * y + 1 - c
    far = 2 * (1 - y) + c
    far_core = 2 * (1 - y) + 1 - c
    count, width = tok.shape
    lane = V
    bf16, f32 = jnp.bfloat16, jnp.float32
    experts, hidden = wg.shape[0], wg.shape[2]
    slots = gate.shape[0]
    filled = n_sp * CAP
    mine = lanes(tp, width)

    pairs = (
        (kn_h, kn), (vn_h, vn), (kb_h, kb), (vb_h, vb), (qn_h, qn), (qb_h, qb),
        (ids_h, ids), (gates_h, gates), (lam_h, lam), (gains_h, gains),
        (tok_h.at[:, mine], tok), (one_h.at[:, mine], gain_one), (two_h, gain_two),
        (pn_h, proj_n), (pb_h, proj_b),
    )
    copies = [pltpu.make_async_copy(a, b, local.at[i]) for i, (a, b) in enumerate(pairs)]
    for copy in copies:
        copy.start()

    def load(e, go):
        for i, (a, b) in enumerate(((wg, gate), (wu, up), (wd, down))):
            slot = lax.rem(e, slots)
            copy = pltpu.make_async_copy(a.at[e], b.at[slot], loaded.at[i, slot])
            copy.start() if go else copy.wait()

    def each(body):
        lax.fori_loop(0, experts, lambda e, _: (body(e), 0)[1], 0)

    lax.fori_loop(0, slots, lambda e, _: (load(e, True), 0)[1], 0)
    greet(n_sp, n_tp, sp, tp)

    def group_of(s):
        return lax.rem(s + s // 2, 2)

    def block_rows(s):
        return pl.ds(pl.multiple_of(s * count, count), count)

    rows = block_rows(sp)

    def piece(grp, head, i):
        size = lane * (1 if i == 2 else grp + 1)
        source = ((qn, kn, vn), (qb, kb, vb))[grp][i]
        return source.at[:, lanes(head, size)]

    def landing(grp, s, i):
        if i == 2:
            return v_all.at[block_rows(s)]
        return (q_all, k_all)[i].at[block_rows(s), 0 : lane * (grp + 1)]

    def qkv(grp, k, i):
        to = flip(sp, k)
        return remote(
            piece(grp, to // 2, i), landing(grp, sp, i), send.at[i, k], recv.at[i, k], "sp", to
        )

    def arrived(grp, k, i):
        source = flip(sp, k)
        block = landing(grp, source, i)
        remote(block, block, send.at[i, k], recv.at[i, k], "sp", source).wait_recv()

    my_group, my_head = group_of(sp), sp // 2

    def send_all(parts):
        for k in range(1, n_sp):
            for grp in range(2):

                @pl.when(group_of(flip(sp, k)) == grp)
                def _():
                    for i in parts:
                        qkv(grp, k, i).start()

    for copy in copies[:4]:
        copy.wait()
    send_all((1, 2))
    for copy in copies[4:6]:
        copy.wait()
    send_all((0,))
    for grp in range(2):

        @pl.when(my_group == grp)
        def _():
            for i in range(3):
                landing(grp, sp, i)[...] = piece(grp, my_head, i)[...]

    for copy in copies[6:13]:
        copy.wait()
    route(ids, gates, spread, shares, n_sp * experts)

    for grp in range(2):

        @pl.when(my_group == grp)
        def _():
            for k in range(1, n_sp):
                arrived(grp, k, 1)
                arrived(grp, k, 2)

    factor = jnp.where(my_group == 0, QK_NARROW**-0.5, QK_BROAD**-0.5) * LOG2E
    lam_row = lam[pl.ds(my_group, 1), :]
    mixing = jnp.sum(
        jnp.where(lax.broadcasted_iota(jnp.int32, lam_row.shape, 1) == my_head, lam_row, 0.0),
        -1,
        keepdims=True,
    )
    gain = gains[pl.ds(my_group, 1), :]
    span = 2 * count
    col = my_group * heads + my_head
    keep_all = jnp.broadcast_to(my_group, (span, lane)) == 1
    place = lax.broadcasted_iota(jnp.int32, (span, lane), 1) // QK_NARROW

    def head_send_of(k):
        s = flip(sp, k)
        return remote(
            head_out.at[block_rows(s), :], head_in.at[:, lanes(col, lane)],
            head_send.at[k], head_recv.at[k], "sp", s,
        )

    for j in range(n_sp // 2):
        first = flip(sp // 2, j)
        q_rows = pl.ds(pl.multiple_of(first * span, span), span)
        for grp in range(2):

            @pl.when(my_group == grp)
            def _():
                for k in (2 * j, 2 * j + 1):
                    if k:
                        arrived(grp, k, 0)

        parts = []
        for m in range(2):
            cut = lanes(my_group * m, lane)
            queries = q_all[q_rows, cut].astype(f32)
            queries = jnp.where(keep_all | (place == m), queries, 0.0).astype(bf16)
            scores = lax.dot_general(
                queries, k_all[:, cut], (((1,), (1,)), ((), ())), preferred_element_type=f32
            )
            highest = jnp.max(scores, -1, keepdims=True)
            expo = jnp.exp2((scores - highest) * factor)
            total = jnp.sum(expo, -1, keepdims=True)
            numer = jnp.dot(expo.astype(bf16), v_all[...], preferred_element_type=f32)
            parts.append(numer / total)
        diff = parts[0] - mixing * parts[1]
        normed = diff * lax.rsqrt(jnp.mean(diff * diff, -1, keepdims=True) + norm_eps) * gain
        head_out[q_rows, :] = normed.astype(bf16)
        for k in (2 * j, 2 * j + 1):
            if k:
                head_send_of(k).start()
            else:
                head_in[:, lanes(col, lane)] = head_out[rows, :]

    for copy in copies[13:]:
        copy.wait()

    def head_arrived(k):
        s = flip(sp, k)
        target = head_in.at[:, lanes(group_of(s) * heads + s // 2, lane)]
        remote(target, target, head_send.at[k], head_recv.at[k], "sp", s).wait_recv()

    side = heads * lane // 2
    half = sp // (n_sp // 2)

    def projected(which, cut):
        at = pl.ds(pl.multiple_of(which * side, side), side)
        wide = pl.ds(pl.multiple_of(which * side + 2 * side, side), side)
        return jnp.dot(head_in[:, at], proj_n[at, cut], preferred_element_type=f32) + jnp.dot(
            head_in[:, wide], proj_b[at, cut], preferred_element_type=f32
        )

    for k in range(1, n_sp // 2):
        head_arrived(k)
    for t in range(n_tp):
        cut = slice(t * width, (t + 1) * width)
        early[:, cut] = projected(half, cut)
    for k in range(n_sp // 2, n_sp):
        head_arrived(k)

    def quarter(t):
        cut = lanes(t, width)
        return early[:, cut] + projected(1 - half, cut)

    def to_partner(i):
        return remote(pc_out.at[i], pc_in.at[i], pc_send.at[i], pc_recv.at[i], "tp", core)

    def partner(i):
        remote(pc_in.at[i], pc_in.at[i], pc_send.at[i], pc_recv.at[i], "tp", core).wait_recv()
        return pc_in[i].astype(f32)

    over = remote(py_out, py_in, py_send.at[0], py_recv.at[0], "tp", far)
    pc_out[0] = quarter(far_core).astype(bf16)
    to_partner(0).start()
    product = quarter(far)
    pc_out[1] = quarter(core).astype(bf16)
    to_partner(1).start()
    py_out[...] = (product + partner(0)).astype(bf16)
    over.start()
    summed_own = quarter(tp) + partner(1) + deep_alpha * tok[...].astype(f32)
    over.wait_recv()
    full = summed_own + py_in[...].astype(f32)

    center = jnp.mean(full, -1, keepdims=True)
    apart = full - center
    squares = jnp.sum(apart * apart, -1, keepdims=True)
    which = lax.broadcasted_iota(jnp.int32, (count, lane), 1)
    st_out[...] = jnp.where(which == 0, center, squares).T[: st_out.shape[0]]

    def share_stats(k):
        to = lax.rem(tp + k, n_tp)
        return remote(st_out, st_in.at[k], st_send.at[k], st_recv.at[k], "tp", to)

    for k in range(1, n_tp):
        share_stats(k).start()
    st_in[0] = st_out[...]
    for k in range(1, n_tp):
        share_stats(k).wait_recv()
    means = [st_in[k, 0:1, :] for k in range(n_tp)]
    mean = sum(means[1:], means[0]) / n_tp
    spreads = [
        st_in[k, 1:2, :] + width * jnp.square(means[k] - mean) for k in range(n_tp)
    ]
    scale = lax.rsqrt(sum(spreads[1:], spreads[0]) / (n_tp * width) + norm_eps)
    upright = jnp.where(
        lax.broadcasted_iota(jnp.int32, (lane, count), 0) == 0, mean, scale
    ).T
    mixed[...] = ((full - upright[:, 0:1]) * upright[:, 1:2] * gain_one[...]).astype(bf16)

    picked = jnp.dot(spread[...], mixed[...], preferred_element_type=f32)
    rows_out[...] = picked.astype(bf16).reshape(rows_out.shape)

    def dispatch(e, k):
        to = flip(sp, k)
        return remote(
            rows_out.at[to, e], rows_in.at[tp, e, sp], a_send.at[e, k], a_recv.at[e, k], "sp", to
        )

    def send_rows(e):
        for k in range(1, n_sp):
            dispatch(e, k).start()
        rows_in[tp, e, sp] = rows_out[sp, e]

    each(send_rows)

    def over_y(e):
        block = rows_in.at[tp, e]
        return remote(block, block, y_send.at[e], y_recv.at[e], "tp", far)

    def across(e, k):
        block = rows_in.at[(tp, far)[k], e]
        return remote(block, block, c_send.at[e, k], c_recv.at[e, k], "tp", core)

    def pass_on(e):
        for k in range(1, n_sp):
            source = flip(sp, k)
            block = rows_in.at[tp, e, source]
            remote(block, block, a_send.at[e, k], a_recv.at[e, k], "sp", source).wait_recv()
        over_y(e).start()
        across(e, 0).start()

    def pass_across(e):
        block = rows_in.at[far, e]
        remote(block, block, y_send.at[e], y_recv.at[e], "tp", far).wait_recv()
        across(e, 1).start()

    def ready(e):
        for k, t in enumerate((core, far_core)):
            block = rows_in.at[t, e]
            remote(block, block, c_send.at[e, k], c_recv.at[e, k], "tp", core).wait_recv()

    def to_core(e, k):
        t = (core, far_core)[k]
        return remote(
            part.at[t, e], part_core.at[k, e], d_send.at[e, k], d_recv.at[e, k], "tp", core
        )

    def to_far(e):
        return remote(part.at[far, e], part_far.at[e], s_send.at[e], s_recv.at[e], "tp", far)

    def give_back(e, k):
        to = flip(sp, k)
        return remote(
            summed.at[e, to], back.at[sp, e], b_send.at[e, k], b_recv.at[e, k], "sp", to
        )

    def core_sum(e, k):
        block = part_core.at[k, e]
        remote(block, block, d_send.at[e, k], d_recv.at[e, k], "tp", core).wait_recv()
        return part[(tp, far)[k], e].astype(f32) + part_core[k, e].astype(f32)

    def reduce_core(e):
        part[far, e] = core_sum(e, 1).astype(bf16)
        to_far(e).start()

    def reduce_far(e):
        total = core_sum(e, 0)
        block = part_far.at[e]
        remote(block, block, s_send.at[e], s_recv.at[e], "tp", far).wait_recv()
        total = total + part_far[e].astype(f32)
        summed[e] = total.astype(bf16).reshape(n_sp, CAP, width)
        for k in range(1, n_sp):
            give_back(e, k).start()
        back[sp, e] = summed[e, sp]

    tile = min(256, hidden)
    tiles = hidden // tile

    def compute(e, _):
        slot = lax.rem(e, slots)
        load(e, False)
        ready(e)
        inputs = jnp.concatenate(
            [rows_in[t, e].reshape(filled, width) for t in range(n_tp)], axis=1
        )

        def hidden_tile(j, _):
            cut = lanes(j, tile)
            gated = jnp.dot(inputs, gate[slot, :, cut], preferred_element_type=f32)
            lifted = jnp.dot(inputs, up[slot, :, cut], preferred_element_type=f32)
            act[:, cut] = (gated / (1.0 + jnp.exp(-gated)) * lifted).astype(bf16)
            pl.when((j == 0) & (e + 2 < experts))(lambda: pass_on(e + 2))
            pl.when((j == min(1, tiles - 1)) & (e >= 2))(lambda: reduce_far(e - 2))
            pl.when((j == min(2, tiles - 1)) & (e + 1 < experts))(lambda: pass_across(e + 1))
            return 0

        lax.fori_loop(0, tiles, hidden_tile, 0)

        def down_tile(i, _):
            t = 2 * lax.rem(y + 1 + i // 2, 2) + lax.rem(c + 1 + i, 2)
            product = jnp.dot(
                act[...], down[slot, :, lanes(t, width)], preferred_element_type=f32
            )
            part[t, e] = product.astype(bf16)
            pl.when(i == 0)(lambda: to_core(e, 1).start())
            pl.when(i == 2)(lambda: to_core(e, 0).start())
            return 0

        lax.fori_loop(0, n_tp, down_tile, 0)
        pl.when(e + slots < experts)(lambda: load(e + slots, True))
        reduce_core(e)
        return 0

    pass_on(0)
    if experts > 1:
        pass_on(1)
    pass_across(0)
    lax.fori_loop(0, experts, compute, 0)
    for e in range(max(0, experts - 2), experts):
        reduce_far(e)

    def arrive(e):
        for k in range(1, n_sp):
            source = flip(sp, k)
            block = back.at[source, e]
            remote(block, block, b_send.at[e, k], b_recv.at[e, k], "sp", source).wait_recv()

    each(arrive)
    returned = back[...].reshape(n_sp * experts * CAP, width)
    routed = jnp.dot(shares[...], returned, preferred_element_type=f32)
    z_all[tp] = (deep_alpha * mixed[...].astype(f32) + routed).astype(bf16)

    def final(i):
        t, to = ((tp, far), (tp, core), (far, core))[i]
        return remote(z_all.at[t], z_all.at[t], g_send.at[i], g_recv.at[i], "tp", to)

    def final_wait(i):
        t, source = ((far, far), (core, core), (far_core, core))[i]
        remote(z_all.at[t], z_all.at[t], g_send.at[i], g_recv.at[i], "tp", source).wait_recv()

    final(0).start()
    final(1).start()
    final_wait(0)
    final(2).start()
    final_wait(1)
    final_wait(2)
    members = [z_all[t].astype(f32) for t in range(n_tp)]
    sums = [jnp.sum(z, -1, keepdims=True) for z in members]
    middle = sum(sums[1:], sums[0]) / (n_tp * width)
    members = [z - middle for z in members]
    sums = [jnp.sum(z * z, -1, keepdims=True) for z in members]
    stretch = lax.rsqrt(sum(sums[1:], sums[0]) / (n_tp * width) + norm_eps)
    for t in range(n_tp):
        cut = slice(t * width, (t + 1) * width)
        out[:, cut] = (members[t] * stretch * gain_two[:, cut]).astype(bf16)

    for k in range(1, n_sp):
        for grp in range(2):

            @pl.when(group_of(flip(sp, k)) == grp)
            def _():
                for i in range(3):
                    qkv(grp, k, i).wait_send()

        head_send_of(k).wait_send()
    for i in range(2):
        to_partner(i).wait_send()
    over.wait_send()
    for k in range(1, n_tp):
        share_stats(k).wait_send()

    def sent(e):
        for k in range(1, n_sp):
            dispatch(e, k).wait_send()
            give_back(e, k).wait_send()
        over_y(e).wait_send()
        for k in range(2):
            across(e, k).wait_send()
            to_core(e, k).wait_send()
        to_far(e).wait_send()

    each(sent)
    for i in range(3):
        final(i).wait_send()


def layer_rows(
    tokens, qn, kn, vn, qb, kb, vb, mix_lambda, head_gain, proj_n, proj_b, gain_one, gain_two,
    expert_ids, expert_gates, wg, wu, wd,
):
    n_sp, n_tp = lax.axis_size("sp"), lax.axis_size("tp")
    count, model_width = tokens.shape
    heads = vn.shape[1] // V
    width = model_width // n_tp
    experts, hidden = wg.shape[0], wg.shape[2]
    slots = min(3, experts)
    filled = n_sp * CAP
    places = n_sp * experts * CAP
    bf16, f32 = jnp.bfloat16, jnp.float32
    dma = pltpu.SemaphoreType.DMA
    far = pl.BlockSpec(memory_space=pltpu.HBM)
    near = pl.BlockSpec(memory_space=pltpu.VMEM)
    vmem = lambda *shape: pltpu.VMEM(shape, bf16)
    wide = lambda *shape: pltpu.VMEM(shape, f32)
    like = lambda array: pltpu.VMEM(array.shape, array.dtype)
    ids, gates = expert_ids.T, expert_gates.T
    one, two = gain_one[None, :], gain_two[None, :]
    operands = (
        mix_lambda, ids, gates, tokens, qn, kn, vn, qb, kb, vb, head_gain, proj_n, proj_b,
        one, two, wg, wu, wd,
    )
    return pl.pallas_call(
        functools.partial(layer_kernel, n_sp, n_tp, heads),
        out_shape=jax.ShapeDtypeStruct(tokens.shape, bf16),
        in_specs=[far] * len(operands),
        out_specs=near,
        scratch_shapes=[
            like(mix_lambda),
            like(ids),
            like(gates),
            vmem(count, width),
            like(qn),
            like(kn),
            like(vn),
            like(qb),
            like(kb),
            like(vb),
            like(head_gain),
            like(proj_n),
            like(proj_b),
            wide(1, width),
            like(two),
            vmem(slots, *wg.shape[1:]),
            vmem(slots, *wu.shape[1:]),
            vmem(slots, *wd.shape[1:]),
            vmem(n_sp * count, 2 * V),
            vmem(n_sp * count, 2 * V),
            vmem(n_sp * count, V),
            vmem(n_sp * count, V),
            vmem(count, 2 * heads * V),
            wide(count, model_width),
            vmem(2, count, width),
            vmem(2, count, width),
            vmem(count, width),
            vmem(count, width),
            wide(8, count),
            wide(n_tp, 8, count),
            vmem(count, width),
            vmem(places, count),
            vmem(count, places),
            vmem(n_sp, experts, CAP, width),
            vmem(n_tp, experts, n_sp, CAP, width),
            vmem(filled, hidden),
            vmem(n_tp, experts, filled, width),
            vmem(2, experts, filled, width),
            vmem(experts, filled, width),
            vmem(experts, n_sp, CAP, width),
            vmem(n_sp, experts, CAP, width),
            vmem(n_tp, count, width),
            dma((15,)),
            dma((3, slots)),
            dma((3, n_sp)),
            dma((3, n_sp)),
            dma((n_sp,)),
            dma((n_sp,)),
        ]
        + [dma((2,))] * 2
        + [dma((1,))] * 2
        + [dma((n_tp,))] * 2
        + [dma((experts, n_sp))] * 2
        + [dma((experts,))] * 2
        + [dma((experts, 2))] * 4
        + [dma((experts,))] * 2
        + [dma((experts, n_sp))] * 2
        + [dma((3,))] * 2,
        compiler_params=pltpu.CompilerParams(
            collective_id=0, has_side_effects=True, vmem_limit_bytes=61 * 2**20
        ),
        name="layer",
    )(*operands)


def head_fold(running, queries, key_rows, values, key_width):
    maxima, totals, weighted = running
    length = key_rows.shape[0]
    head_count = queries.shape[1]
    keyed = key_rows.reshape(length, head_count, 2, key_width)
    valued = values.reshape(length, head_count, V)
    scores = jnp.einsum(
        "qhmd,khmd->hmqk", queries, keyed, preferred_element_type=jnp.float32
    ) * key_width ** (-0.5)
    updated = jnp.maximum(maxima, jnp.max(scores, -1))
    exponent = jnp.exp(scores - updated[..., None])
    totals = jnp.sum(exponent, -1)
    weighted = jnp.einsum(
        "hmqk,khv->hmqv", exponent.astype(jnp.bfloat16), valued, preferred_element_type=jnp.float32
    )
    return (updated, totals, weighted)


def head_output(running, mixing, gains):
    maxima, totals, weighted = running
    diff = (
        weighted[:, 0] / totals[:, 0, :, None]
        - mixing[:, None, None] * weighted[:, 1] / totals[:, 1, :, None]
    )
    normed = (diff * lax.rsqrt(jnp.mean(diff * diff, -1, keepdims=True) + norm_eps) * gains).astype(
        jnp.bfloat16
    )
    return jnp.moveaxis(normed, 0, 1).reshape(normed.shape[1], -1)


def attention_gathered(
    tokens,
    query_narrow,
    key_narrow,
    value_narrow,
    query_broad,
    key_broad,
    value_broad,
    mix_lambda,
    head_gain,
    proj_narrow,
    proj_broad,
    gain_one,
):
    token_count = tokens.shape[0]
    head_count = value_narrow.shape[1] // V
    queries_first = query_narrow.reshape(token_count, head_count, 2, QK_NARROW)
    queries_second = query_broad.reshape(token_count, head_count, 2, QK_BROAD)
    start_state = (
        jnp.full((head_count, 2, token_count), -1e30, jnp.float32),
        jnp.zeros((head_count, 2, token_count), jnp.float32),
        jnp.zeros((head_count, 2, token_count, V), jnp.float32),
    )
    state_first = head_fold(
        start_state,
        queries_first,
        lax.all_gather(key_narrow, "sp", axis=0, tiled=True),
        lax.all_gather(value_narrow, "sp", axis=0, tiled=True),
        QK_NARROW,
    )
    state_second = head_fold(
        start_state,
        queries_second,
        lax.all_gather(key_broad, "sp", axis=0, tiled=True),
        lax.all_gather(value_broad, "sp", axis=0, tiled=True),
        QK_BROAD,
    )
    heads_first = head_output(state_first, mix_lambda[0], head_gain[0])
    heads_second = head_output(state_second, mix_lambda[1], head_gain[1])
    partial_value = jnp.dot(heads_first, proj_narrow, preferred_element_type=jnp.float32)
    partial_value = partial_value + jnp.dot(
        heads_second, proj_broad, preferred_element_type=jnp.float32
    )
    attn = lax.psum(
        partial_value.astype(jnp.bfloat16).astype(jnp.float32).astype(jnp.bfloat16), "tp"
    ).astype(jnp.float32)
    return layer_scale(deep_alpha * tokens.astype(jnp.float32) + attn, gain_one).astype(
        jnp.bfloat16
    )


def on_device(
    tokens,
    query_narrow,
    key_narrow,
    value_narrow,
    query_broad,
    key_broad,
    value_broad,
    mix_lambda,
    head_gain,
    proj_narrow,
    proj_broad,
    gain_one,
    gain_two,
    expert_ids,
    expert_gates,
    gate_weight,
    up_weight,
    down_weight,
):
    token_count = tokens.shape[0]
    model_width = tokens.shape[1]
    members = (
        tokens,
        query_narrow,
        key_narrow,
        value_narrow,
        query_broad,
        key_broad,
        value_broad,
        mix_lambda,
        head_gain,
        proj_narrow,
        proj_broad,
        gain_one,
    )
    n_sp, n_tp = lax.axis_size("sp"), lax.axis_size("tp")
    whole_heads = 2 * (value_narrow.shape[1] // V) == n_sp
    if whole_heads and n_tp // 2 == 2 and not n_sp & (n_sp - 1):
        return layer_rows(
            *members, gain_two, expert_ids, expert_gates, gate_weight, up_weight, down_weight
        )
    mixed_rows = attention_gathered(*members)
    experts_all = gate_weight.shape[0] * lax.axis_size("sp")
    chosen = expert_ids.reshape(-1)
    onehot = (chosen[:, None] == jnp.arange(experts_all, dtype=jnp.int32)[None, :]).astype(
        jnp.int32
    )
    before = jnp.cumsum(onehot, axis=0, dtype=jnp.int32) - onehot
    slot_index = jnp.sum(before * onehot, axis=-1, dtype=jnp.int32)
    position = (chosen * CAP + slot_index).reshape(expert_ids.shape)
    match = position[:, :, None] == jnp.arange(CAP * experts_all, dtype=jnp.int32)
    spread = jnp.any(match, axis=1).astype(jnp.bfloat16).T
    shares = jnp.sum(jnp.where(match, expert_gates[:, :, None], 0.0), axis=1)
    high = lax.reduce_precision(shares, 8, 7)
    low = (shares - high).astype(jnp.bfloat16)
    return expert_rows(
        mixed_rows,
        spread,
        high.astype(jnp.bfloat16),
        low,
        gain_two,
        gate_weight,
        up_weight,
        down_weight,
    )


def solution(mesh):
    return jax.shard_map(
        on_device,
        mesh=mesh,
        in_specs=(
            P("sp", None),
            P("sp", "tp"),
            P("sp", "tp"),
            P("sp", "tp"),
            P("sp", "tp"),
            P("sp", "tp"),
            P("sp", "tp"),
            P(None, "tp"),
            P(),
            P("tp", None),
            P("tp", None),
            P(),
            P(),
            P("sp", None),
            P("sp", None),
            P("sp", None, "tp"),
            P("sp", None, "tp"),
            P("sp", "tp", None),
        ),
        out_specs=P("sp", None),
        check_vma=False,
    )
```

```python
import functools

import jax
import jax.numpy as jnp
from jax import lax
from jax.experimental import pallas as pl
from jax.experimental.pallas import tpu as pltpu
from jax.sharding import PartitionSpec as P

QK_NARROW = 64
QK_BROAD = 128
V = 128
TOP = 2
CAP = 16


deep_alpha = 8.0**0.25
norm_eps = 1e-05


def layer_scale(inputs, gains):
    center = jnp.mean(inputs, -1, keepdims=True)
    spread = jnp.mean(jnp.square(inputs - center), -1, keepdims=True)
    return (inputs - center) * lax.rsqrt(spread + norm_eps) * gains


MESH = pl.DeviceIdType.MESH
LOG2E = 1.4426950408889634


def remote(src, dst, send, recv, axis, index):
    return pltpu.make_async_remote_copy(
        src_ref=src,
        dst_ref=dst,
        send_sem=send,
        recv_sem=recv,
        device_id={axis: index},
        device_id_type=MESH,
    )


def greet(n_sp, n_tp, sp, tp):
    barrier = pltpu.get_barrier_semaphore()
    for k in range(1, n_sp):
        pl.semaphore_signal(
            barrier, inc=1, device_id={"sp": lax.rem(sp + k, n_sp)}, device_id_type=MESH
        )
    for k in range(1, n_tp):
        pl.semaphore_signal(
            barrier, inc=1, device_id={"tp": lax.rem(tp + k, n_tp)}, device_id_type=MESH
        )
    pl.semaphore_wait(barrier, n_sp + n_tp - 2)


def lanes(index, width):
    return pl.ds(pl.multiple_of(index * width, width), width)


def expert_kernel(
    n_sp, n_tp, mixed, spread, high, low, gain_two, wg, wu, wd, out,
    gate, up, down, rows_out, rows_in, act, part, part_core, part_far, summed, back, routed,
    loaded, a_send, a_recv, y_send, y_recv, c_send, c_recv,
    d_send, d_recv, s_send, s_recv, b_send, b_recv, g_send, g_recv,
):
    sp, tp = lax.axis_index("sp"), lax.axis_index("tp")
    experts, slots, width = rows_out.shape[1:]
    hidden = act.shape[1]
    filled = n_sp * slots
    pairs = n_tp // 2
    y, c = tp // 2, tp % 2
    other = 2 * y + 1 - c

    def load(e, go):
        for i, (a, b) in enumerate(((wg, gate), (wu, up), (wd, down))):
            copy = pltpu.make_async_copy(a.at[e], b.at[e], loaded.at[i, e])
            copy.start() if go else copy.wait()

    def each(body):
        lax.fori_loop(0, experts, lambda e, _: (body(e), 0)[1], 0)

    each(lambda e: load(e, True))
    greet(n_sp, n_tp, sp, tp)

    mine = lanes(tp, width)
    picked = jnp.dot(spread[...], mixed[:, mine], preferred_element_type=jnp.float32)
    rows_out[...] = picked.astype(jnp.bfloat16).reshape(rows_out.shape)

    def dispatch(e, k):
        to = lax.rem(sp + k, n_sp)
        return remote(
            rows_out.at[to, e], rows_in.at[tp, e, sp], a_send.at[e, k], a_recv.at[e, k], "sp", to
        )

    def send_rows(e):
        for k in range(1, n_sp):
            dispatch(e, k).start()
        rows_in[tp, e, sp] = rows_out[sp, e]

    each(send_rows)

    def far(e, k):
        block = rows_in.at[tp, e]
        to = 2 * lax.rem(y + k, pairs) + c
        return remote(block, block, y_send.at[e, k], y_recv.at[e, k], "tp", to)

    def far_slot(k):
        return 2 * lax.rem(y + pairs - k, pairs) + c

    def across(e, k):
        block = rows_in.at[far_slot(k), e]
        return remote(block, block, c_send.at[e, k], c_recv.at[e, k], "tp", other)

    def pass_on(e):
        for k in range(1, n_sp):
            source = lax.rem(sp + n_sp - k, n_sp)
            block = rows_in.at[tp, e, source]
            remote(block, block, a_send.at[e, k], a_recv.at[e, k], "sp", source).wait_recv()
        for k in range(1, pairs):
            far(e, k).start()
        across(e, 0).start()

    each(pass_on)

    def pass_across(e):
        for k in range(1, pairs):
            block = rows_in.at[far_slot(k), e]
            remote(block, block, y_send.at[e, k], y_recv.at[e, k], "tp", far_slot(k)).wait_recv()
            across(e, k).start()

    def to_core(e, k):
        yy = lax.rem(y + k, pairs)
        return remote(
            part.at[2 * yy + 1 - c, e], part_core.at[k, e], d_send.at[e, k], d_recv.at[e, k],
            "tp", other,
        )

    def to_far(e, k):
        to = 2 * lax.rem(y + k, pairs) + c
        return remote(
            part.at[to, e], part_far.at[k, e], s_send.at[e, k], s_recv.at[e, k], "tp", to
        )

    def give_back(e, k):
        to = lax.rem(sp + k, n_sp)
        return remote(
            summed.at[e, to], back.at[sp, e], b_send.at[e, k], b_recv.at[e, k], "sp", to
        )

    tile = min(256, hidden)

    def compute(e):
        pass_across(e)
        load(e, False)
        for k in range(pairs):
            block = rows_in.at[2 * lax.rem(y + pairs - k, pairs) + 1 - c, e]
            remote(block, block, c_send.at[e, k], c_recv.at[e, k], "tp", other).wait_recv()
        inputs = jnp.concatenate(
            [rows_in[t, e].reshape(filled, width) for t in range(n_tp)], axis=1
        )

        def hidden_tile(j, _):
            cut = lanes(j, tile)
            gated = jnp.dot(inputs, gate[e, :, cut], preferred_element_type=jnp.float32)
            lifted = jnp.dot(inputs, up[e, :, cut], preferred_element_type=jnp.float32)
            act[:, cut] = (gated / (1.0 + jnp.exp(-gated)) * lifted).astype(jnp.bfloat16)
            return 0

        lax.fori_loop(0, hidden // tile, hidden_tile, 0)

        def down_tile(t, _):
            product = jnp.dot(
                act[...], down[e, :, lanes(t, width)], preferred_element_type=jnp.float32
            )
            part[t, e] = product.astype(jnp.bfloat16)
            return 0

        lax.fori_loop(0, n_tp, down_tile, 0)
        for k in range(pairs):
            to_core(e, k).start()

    def core_sum(e, k):
        block = part_core.at[k, e]
        remote(block, block, d_send.at[e, k], d_recv.at[e, k], "tp", other).wait_recv()
        slot = 2 * lax.rem(y + k, pairs) + c
        return part[slot, e].astype(jnp.float32) + part_core[k, e].astype(jnp.float32)

    def reduce_core(e):
        for k in range(1, pairs):
            total = core_sum(e, k)
            part[2 * lax.rem(y + k, pairs) + c, e] = total.astype(jnp.bfloat16)
            to_far(e, k).start()

    def reduce_far(e):
        total = core_sum(e, 0)
        for k in range(1, pairs):
            block = part_far.at[k, e]
            remote(block, block, s_send.at[e, k], s_recv.at[e, k], "tp", far_slot(k)).wait_recv()
            total = total + part_far[k, e].astype(jnp.float32)
        summed[e] = total.astype(jnp.bfloat16).reshape(n_sp, slots, width)
        for k in range(1, n_sp):
            give_back(e, k).start()
        back[sp, e] = summed[e, sp]

    def step(e, _):
        pl.when(e < experts)(lambda: compute(e))
        pl.when((e >= 1) & (e <= experts))(lambda: reduce_core(e - 1))
        pl.when(e >= 2)(lambda: reduce_far(e - 2))
        return 0

    lax.fori_loop(0, experts + 2, step, 0)

    def arrive(e):
        for k in range(1, n_sp):
            source = lax.rem(sp + n_sp - k, n_sp)
            block = back.at[source, e]
            remote(block, block, b_send.at[e, k], b_recv.at[e, k], "sp", source).wait_recv()

    each(arrive)
    returned = back[...].reshape(n_sp * experts * slots, width)
    weighted = jnp.dot(high[...], returned, preferred_element_type=jnp.float32) + jnp.dot(
        low[...], returned, preferred_element_type=jnp.float32
    )
    routed[:, mine] = weighted.astype(jnp.bfloat16)

    def share(k):
        to = lax.rem(tp + k, n_tp)
        block = routed.at[:, mine]
        return remote(block, block, g_send.at[k], g_recv.at[k], "tp", to)

    for k in range(1, n_tp):
        share(k).start()
    for k in range(1, n_tp):
        peer = lax.rem(tp + n_tp - k, n_tp)
        block = routed.at[:, lanes(peer, width)]
        remote(block, block, g_send.at[k], g_recv.at[k], "tp", peer).wait_recv()
    full = deep_alpha * mixed[...].astype(jnp.float32) + routed[...].astype(jnp.float32)
    out[...] = layer_scale(full, gain_two[...]).astype(jnp.bfloat16)

    def sent(e):
        for k in range(1, n_sp):
            dispatch(e, k).wait_send()
            give_back(e, k).wait_send()
        for k in range(pairs):
            across(e, k).wait_send()
            to_core(e, k).wait_send()
        for k in range(1, pairs):
            far(e, k).wait_send()
            to_far(e, k).wait_send()

    each(sent)
    for k in range(1, n_tp):
        share(k).wait_send()


def expert_rows(mixed, spread, high, low, gain_two, wg, wu, wd):
    n_sp, n_tp = lax.axis_size("sp"), lax.axis_size("tp")
    count, model_width = mixed.shape
    experts, hidden = wg.shape[0], wg.shape[2]
    width, pairs, filled = model_width // n_tp, n_tp // 2, n_sp * CAP
    bf16 = jnp.bfloat16
    dma = pltpu.SemaphoreType.DMA
    far = pl.BlockSpec(memory_space=pl.ANY)
    near = pl.BlockSpec(memory_space=pltpu.VMEM)
    vmem = lambda *shape: pltpu.VMEM(shape, bf16)
    return pl.pallas_call(
        functools.partial(expert_kernel, n_sp, n_tp),
        out_shape=jax.ShapeDtypeStruct(mixed.shape, bf16),
        in_specs=[near] * 5 + [far] * 3,
        out_specs=near,
        scratch_shapes=[
            vmem(*wg.shape),
            vmem(*wu.shape),
            vmem(*wd.shape),
            vmem(n_sp, experts, CAP, width),
            vmem(n_tp, experts, n_sp, CAP, width),
            vmem(filled, hidden),
            vmem(n_tp, experts, filled, width),
            vmem(pairs, experts, filled, width),
            vmem(pairs, experts, filled, width),
            vmem(experts, n_sp, CAP, width),
            vmem(n_sp, experts, CAP, width),
            vmem(count, model_width),
            dma((3, experts)),
        ]
        + [dma((experts, n_sp))] * 2
        + [dma((experts, pairs))] * 8
        + [dma((experts, n_sp))] * 2
        + [dma((n_tp,))] * 2,
        compiler_params=pltpu.CompilerParams(
            collective_id=1, has_side_effects=True, vmem_limit_bytes=67043328
        ),
        name="experts",
    )(mixed, spread, high, low, gain_two[None, :], wg, wu, wd)


def flip(index, mask):
    bit = 1
    while bit <= mask:
        if mask & bit:
            index = index + bit - 2 * bit * lax.rem(index // bit, 2)
        bit *= 2
    return index


def route(ids, gates, spread, shares, experts_all, owners):
    count = ids.shape[1]
    expert = lax.broadcasted_iota(jnp.int32, (experts_all, count), 0)
    picks = [(expert == ids[k : k + 1, :]).astype(jnp.float32) for k in range(TOP)]
    taken = functools.reduce(lambda a, b: a + b, picks)
    earlier = lax.broadcasted_iota(jnp.int32, (count, count), 0) < lax.broadcasted_iota(
        jnp.int32, (count, count), 1
    )
    before = jnp.dot(
        taken.astype(jnp.bfloat16),
        earlier.astype(jnp.float32).astype(jnp.bfloat16),
        preferred_element_type=jnp.float32,
    )
    place = lax.broadcasted_iota(jnp.int32, (experts_all * CAP, count), 0).astype(jnp.float32)
    weight = jnp.zeros((experts_all * CAP, count), jnp.float32)
    marked = jnp.zeros((experts_all * CAP, count), jnp.float32)
    for k in range(TOP):
        slot = jnp.sum(before * picks[k], 0, keepdims=True)
        chosen, own = ids[k : k + 1, :], experts_all // owners
        order = lax.rem(chosen, own) * owners + chosen // own
        position = order.astype(jnp.float32) * CAP + slot
        hit = place == position
        weight = weight + jnp.where(hit, gates[k : k + 1, :], 0.0)
        marked = marked + jnp.where(hit, 1.0, 0.0)
    spread[...] = marked.astype(jnp.bfloat16)
    shares[...] = weight.T.astype(jnp.bfloat16)


def layer_kernel(
    n_sp, n_tp, heads, lam_h, ids_h, gates_h, tok_h, qn_h, kn_h, vn_h, qb_h, kb_h, vb_h,
    gains_h, pn_h, pb_h, one_h, two_h, wg, wu, wd, out,
    lam, ids, gates, tok, qn, kn, vn, qb, kb, vb, gains, proj_n, proj_b, gain_one, gain_two,
    gate, up, down, q_all, k_all, v_all, head_out, head_in, early, pc_out, pc_in, py_out, py_in,
    st_out, st_in, mixed, spread, shares, rows_out, rows_in, act, part, part_core, part_far,
    summed, back, z_all,
    local, loaded, send, recv, head_send, head_recv, pc_send, pc_recv, py_send, py_recv,
    st_send, st_recv, a_send, a_recv, y_send, y_recv, c_send, c_recv, d_send, d_recv,
    s_send, s_recv, b_send, b_recv, g_send, g_recv,
):
    sp, tp = lax.axis_index("sp"), lax.axis_index("tp")
    y, c = tp // 2, lax.rem(tp, 2)
    core = 2 * y + 1 - c
    far = 2 * (1 - y) + c
    far_core = 2 * (1 - y) + 1 - c
    count, width = tok.shape
    lane = V
    bf16, f32 = jnp.bfloat16, jnp.float32
    experts, hidden = wg.shape[0], wg.shape[2]
    slots = gate.shape[0]
    filled = n_sp * CAP
    mine = lanes(tp, width)

    pairs = (
        (kn_h, kn), (vn_h, vn), (kb_h, kb), (vb_h, vb), (qn_h, qn), (qb_h, qb),
        (ids_h, ids), (gates_h, gates), (lam_h, lam), (gains_h, gains),
        (tok_h.at[:, mine], tok), (one_h.at[:, mine], gain_one), (two_h, gain_two),
        (pn_h, proj_n), (pb_h, proj_b),
    )
    copies = [pltpu.make_async_copy(a, b, local.at[i]) for i, (a, b) in enumerate(pairs)]
    for copy in copies:
        copy.start()

    def load(e, go):
        for i, (a, b) in enumerate(((wg, gate), (wu, up), (wd, down))):
            slot = lax.rem(e, slots)
            copy = pltpu.make_async_copy(a.at[e], b.at[slot], loaded.at[i, slot])
            copy.start() if go else copy.wait()

    def each(body):
        lax.fori_loop(0, experts, lambda e, _: (body(e), 0)[1], 0)

    lax.fori_loop(0, slots, lambda e, _: (load(e, True), 0)[1], 0)
    greet(n_sp, n_tp, sp, tp)

    def group_of(s):
        return lax.rem(s + s // 2, 2)

    def block_rows(s):
        return pl.ds(pl.multiple_of(s * count, count), count)

    rows = block_rows(sp)

    def piece(grp, head, i):
        size = lane * (1 if i == 2 else grp + 1)
        source = ((qn, kn, vn), (qb, kb, vb))[grp][i]
        return source.at[:, lanes(head, size)]

    def landing(grp, s, i):
        if i == 2:
            return v_all.at[block_rows(s)]
        return (q_all, k_all)[i].at[block_rows(s), 0 : lane * (grp + 1)]

    def qkv(grp, k, i):
        to = flip(sp, k)
        return remote(
            piece(grp, to // 2, i), landing(grp, sp, i), send.at[i, k], recv.at[i, k], "sp", to
        )

    def arrived(grp, k, i):
        source = flip(sp, k)
        block = landing(grp, source, i)
        remote(block, block, send.at[i, k], recv.at[i, k], "sp", source).wait_recv()

    my_group, my_head = group_of(sp), sp // 2

    near = n_sp // 2
    order = [*range(near - 1, 0, -1), *range(n_sp - 1, near - 1, -1)]

    def side_order(g):
        return order[near - 1 :] if g else order[: near - 1]

    def send_all(parts):
        for k in order:
            for grp in range(2):

                @pl.when(group_of(flip(sp, k)) == grp)
                def _():
                    for i in parts:
                        qkv(grp, k, i).start()

    for copy in copies[:4]:
        copy.wait()
    send_all((1, 2))
    for copy in copies[4:6]:
        copy.wait()
    send_all((0,))
    for grp in range(2):

        @pl.when(my_group == grp)
        def _():
            for i in range(3):
                landing(grp, sp, i)[...] = piece(grp, my_head, i)[...]

    for copy in copies[6:13]:
        copy.wait()
    route(ids, gates, spread, shares, n_sp * experts, n_sp)

    for grp in range(2):

        @pl.when(my_group == grp)
        def _():
            for k in range(1, n_sp):
                arrived(grp, k, 1)
                arrived(grp, k, 2)

    factor = jnp.where(my_group == 0, QK_NARROW**-0.5, QK_BROAD**-0.5) * LOG2E
    lam_row = lam[pl.ds(my_group, 1), :]
    mixing = jnp.sum(
        jnp.where(lax.broadcasted_iota(jnp.int32, lam_row.shape, 1) == my_head, lam_row, 0.0),
        -1,
        keepdims=True,
    )
    gain = gains[pl.ds(my_group, 1), :]
    col = my_group * heads + my_head

    def head_send_of(k):
        s = flip(sp, k)
        return remote(
            head_out.at[block_rows(s), :], head_in.at[:, lanes(col, lane)],
            head_send.at[k], head_recv.at[k], "sp", s,
        )

    def attend(ks):
        for grp in range(2):

            @pl.when(my_group == grp)
            def _():
                for k in ks:
                    if k:
                        arrived(grp, k, 0)

        span = len(ks) * count
        first = flip(sp, ks[0]) // len(ks)
        q_rows = pl.ds(pl.multiple_of(first * span, span), span)
        keep_all = jnp.broadcast_to(my_group, (span, lane)) == 1
        place = lax.broadcasted_iota(jnp.int32, (span, lane), 1) // QK_NARROW
        parts = []
        for m in range(2):
            cut = lanes(my_group * m, lane)
            queries = q_all[q_rows, cut].astype(f32)
            queries = jnp.where(keep_all | (place == m), queries, 0.0).astype(bf16)
            scores = lax.dot_general(
                queries, k_all[:, cut], (((1,), (1,)), ((), ())), preferred_element_type=f32
            )
            highest = jnp.max(scores, -1, keepdims=True)
            expo = jnp.exp2((scores - highest) * factor)
            total = jnp.sum(expo, -1, keepdims=True)
            numer = jnp.dot(expo.astype(bf16), v_all[...], preferred_element_type=f32)
            parts.append(numer / total)
        diff = parts[0] - mixing * parts[1]
        normed = diff * lax.rsqrt(jnp.mean(diff * diff, -1, keepdims=True) + norm_eps) * gain
        head_out[q_rows, :] = normed.astype(bf16)
        for k in ks[::-1]:
            if k:
                head_send_of(k).start()
            else:
                head_in[:, lanes(col, lane)] = head_out[rows, :]

    for k in (*range(0, near, 2), *range(n_sp - 2, near - 1, -2)):
        attend((k, k + 1))

    for copy in copies[13:]:
        copy.wait()

    def head_arrived(k):
        s = flip(sp, k)
        target = head_in.at[:, lanes(group_of(s) * heads + s // 2, lane)]
        remote(target, target, head_send.at[k], head_recv.at[k], "sp", s).wait_recv()

    side = heads * lane // 2
    half = sp // (n_sp // 2)

    def projected(which, cut):
        at = pl.ds(pl.multiple_of(which * side, side), side)
        wide = pl.ds(pl.multiple_of(which * side + 2 * side, side), side)
        return jnp.dot(head_in[:, at], proj_n[at, cut], preferred_element_type=f32) + jnp.dot(
            head_in[:, wide], proj_b[at, cut], preferred_element_type=f32
        )

    for k in range(1, n_sp // 2):
        head_arrived(k)
    for t in range(n_tp):
        cut = slice(t * width, (t + 1) * width)
        early[:, cut] = projected(half, cut)
    for k in range(n_sp // 2, n_sp):
        head_arrived(k)

    def quarter(t):
        cut = lanes(t, width)
        return early[:, cut] + projected(1 - half, cut)

    def to_partner(i):
        return remote(pc_out.at[i], pc_in.at[i], pc_send.at[i], pc_recv.at[i], "tp", core)

    def partner(i):
        remote(pc_in.at[i], pc_in.at[i], pc_send.at[i], pc_recv.at[i], "tp", core).wait_recv()
        return pc_in[i].astype(f32)

    over = remote(py_out, py_in, py_send.at[0], py_recv.at[0], "tp", far)
    pc_out[0] = quarter(far_core).astype(bf16)
    to_partner(0).start()
    product = quarter(far)
    pc_out[1] = quarter(core).astype(bf16)
    to_partner(1).start()
    py_out[...] = (product + partner(0)).astype(bf16)
    over.start()
    summed_own = quarter(tp) + partner(1) + deep_alpha * tok[...].astype(f32)
    over.wait_recv()
    full = summed_own + py_in[...].astype(f32)

    center = jnp.mean(full, -1, keepdims=True)
    apart = full - center
    squares = jnp.sum(apart * apart, -1, keepdims=True)
    which = lax.broadcasted_iota(jnp.int32, (count, lane), 1)
    st_out[...] = jnp.where(which == 0, center, squares).T[: st_out.shape[0]]

    def share_stats(k):
        to = lax.rem(tp + k, n_tp)
        return remote(st_out, st_in.at[k], st_send.at[k], st_recv.at[k], "tp", to)

    for k in range(1, n_tp):
        share_stats(k).start()
    st_in[0] = st_out[...]
    for k in range(1, n_tp):
        share_stats(k).wait_recv()
    means = [st_in[k, 0:1, :] for k in range(n_tp)]
    mean = sum(means[1:], means[0]) / n_tp
    spreads = [
        st_in[k, 1:2, :] + width * jnp.square(means[k] - mean) for k in range(n_tp)
    ]
    scale = lax.rsqrt(sum(spreads[1:], spreads[0]) / (n_tp * width) + norm_eps)
    upright = jnp.where(
        lax.broadcasted_iota(jnp.int32, (lane, count), 0) == 0, mean, scale
    ).T
    mixed[...] = ((full - upright[:, 0:1]) * upright[:, 1:2] * gain_one[...]).astype(bf16)


    def dispatch(e, k):
        to = flip(sp, k)
        return remote(
            rows_out.at[e, to], rows_in.at[tp, e, sp], a_send.at[e, k], a_recv.at[e, k], "sp", to
        )

    def send_rows(e):
        at = pl.ds(pl.multiple_of(e * filled, filled), filled)
        picked = jnp.dot(spread[at, :], mixed[...], preferred_element_type=f32)
        rows_out[e] = picked.astype(bf16).reshape(rows_out.shape[1:])
        for k in order:
            dispatch(e, k).start()
        rows_in[tp, e, sp] = rows_out[e, sp]

    each(send_rows)

    def side_of(g):
        return pl.ds(pl.multiple_of((half if g == 0 else 1 - half) * near, near), near)

    def over_y(e, g):
        block = rows_in.at[tp, e, side_of(g)]
        return remote(block, block, y_send.at[e, g], y_recv.at[e, g], "tp", far)

    def across(e, k, g):
        block = rows_in.at[(tp, far)[k], e, side_of(g)]
        i = 2 * k + g
        return remote(block, block, c_send.at[e, i], c_recv.at[e, i], "tp", core)

    def pass_on(e, g):
        for k in side_order(g):
            source = flip(sp, k)
            block = rows_in.at[tp, e, source]
            remote(block, block, a_send.at[e, k], a_recv.at[e, k], "sp", source).wait_recv()
        over_y(e, g).start()
        across(e, 0, g).start()

    def pass_across(e, g):
        block = rows_in.at[far, e, side_of(g)]
        remote(block, block, y_send.at[e, g], y_recv.at[e, g], "tp", far).wait_recv()
        across(e, 1, g).start()

    def ready(e):
        for k, t in enumerate((core, far_core)):
            for g in range(2):
                block = rows_in.at[t, e, side_of(g)]
                i = 2 * k + g
                remote(block, block, c_send.at[e, i], c_recv.at[e, i], "tp", core).wait_recv()

    def to_core(e, k):
        t = (core, far_core)[k]
        return remote(
            part.at[t, e], part_core.at[k, e], d_send.at[e, k], d_recv.at[e, k], "tp", core
        )

    def rows_for(g):
        size = near * CAP
        return pl.ds(pl.multiple_of((half if g == 0 else 1 - half) * size, size), size)

    def to_far(e, g):
        at = rows_for(g)
        return remote(
            part.at[far, e, at], part_far.at[e, at], s_send.at[e, g], s_recv.at[e, g], "tp", far
        )

    def give_back(e, k):
        to = flip(sp, k)
        return remote(
            summed.at[e, to], back.at[e, sp], b_send.at[e, k], b_recv.at[e, k], "sp", to
        )

    def core_arrived(e, k):
        block = part_core.at[k, e]
        remote(block, block, d_send.at[e, k], d_recv.at[e, k], "tp", core).wait_recv()

    def reduce_core(e, g):
        if g == 1:
            core_arrived(e, 1)
        at = rows_for(g)
        total = part[far, e, at].astype(f32) + part_core[1, e, at].astype(f32)
        part[far, e, at] = total.astype(bf16)
        to_far(e, g).start()

    def reduce_far(e, g):
        if g == 1:
            core_arrived(e, 0)
        at = rows_for(g)
        block = part_far.at[e, at]
        remote(block, block, s_send.at[e, g], s_recv.at[e, g], "tp", far).wait_recv()
        total = part[tp, e, at].astype(f32) + part_core[0, e, at].astype(f32)
        total = total + part_far[e, at].astype(f32)
        summed[e, side_of(g)] = total.astype(bf16).reshape(near, CAP, width)
        for k in side_order(g):
            give_back(e, k).start()
        if g == 0:
            back[e, sp] = summed[e, sp]

    tile = min(512, hidden)
    tiles = hidden // tile

    def compute(e, _):
        slot = lax.rem(e, slots)
        load(e, False)
        ready(e)
        inputs = jnp.concatenate(
            [rows_in[t, e].reshape(filled, width) for t in range(n_tp)], axis=1
        )

        def hidden_tile(j, _):
            cut = lanes(j, tile)
            gated = jnp.dot(inputs, gate[slot, :, cut], preferred_element_type=f32)
            lifted = jnp.dot(inputs, up[slot, :, cut], preferred_element_type=f32)
            act[:, cut] = (gated / (1.0 + jnp.exp(-gated)) * lifted).astype(bf16)
            pl.when(j == 0)(lambda: between(e))
            return 0

        def between(e):
            pl.when(e + 2 < experts)(lambda: pass_on(e + 2, 1))
            pl.when(e + 3 < experts)(lambda: pass_on(e + 3, 0))
            pl.when(e >= 1)(lambda: reduce_core(e - 1, 0))
            pl.when(e >= 2)(lambda: reduce_far(e - 2, 1))

        lax.fori_loop(0, tiles, hidden_tile, 0)
        for g in range(2):
            pl.when(e + 1 < experts)(lambda: pass_across(e + 1, g))
        pl.when(e >= 2)(lambda: reduce_far(e - 2, 0))

        def down_tile(i, _):
            t = 2 * lax.rem(y + 1 + i // 2, 2) + lax.rem(c + 1 + i, 2)
            product = jnp.dot(
                act[...], down[slot, :, lanes(t, width)], preferred_element_type=f32
            )
            part[t, e] = product.astype(bf16)
            pl.when(i == 0)(lambda: to_core(e, 1).start())
            pl.when(i == 2)(lambda: to_core(e, 0).start())
            return 0

        lax.fori_loop(0, n_tp, down_tile, 0)
        pl.when(e + slots < experts)(lambda: load(e + slots, True))
        reduce_core(e, 1)
        return 0

    pass_on(0, 0)
    if experts > 1:
        pass_on(1, 0)
    pass_on(0, 1)
    pass_across(0, 0)
    if experts > 1:
        pass_on(1, 1)
    if experts > 2:
        pass_on(2, 0)
    pass_across(0, 1)
    lax.fori_loop(0, experts, compute, 0)
    reduce_core(experts - 1, 0)
    for g in (1, 0):
        for e in range(max(0, experts - 2), experts):
            reduce_far(e, g)

    def arrive(e, total):
        for k in order:
            source = flip(sp, k)
            block = back.at[e, source]
            remote(block, block, b_send.at[e, k], b_recv.at[e, k], "sp", source).wait_recv()
        at = slice(e * filled, (e + 1) * filled)
        return total + jnp.dot(
            shares[:, at], back[e].reshape(filled, width), preferred_element_type=f32
        )

    total = deep_alpha * mixed[...].astype(f32)
    for e in range(experts):
        total = arrive(e, total)
    z_all[tp] = total.astype(bf16)

    def final(i):
        t, to = ((tp, far), (tp, core), (far, core))[i]
        return remote(z_all.at[t], z_all.at[t], g_send.at[i], g_recv.at[i], "tp", to)

    def final_wait(i):
        t, source = ((far, far), (core, core), (far_core, core))[i]
        remote(z_all.at[t], z_all.at[t], g_send.at[i], g_recv.at[i], "tp", source).wait_recv()

    final(0).start()
    final(1).start()
    final_wait(0)
    final(2).start()
    final_wait(1)
    final_wait(2)
    members = [z_all[t].astype(f32) for t in range(n_tp)]
    sums = [jnp.sum(z, -1, keepdims=True) for z in members]
    middle = sum(sums[1:], sums[0]) / (n_tp * width)
    members = [z - middle for z in members]
    sums = [jnp.sum(z * z, -1, keepdims=True) for z in members]
    stretch = lax.rsqrt(sum(sums[1:], sums[0]) / (n_tp * width) + norm_eps)
    for t in range(n_tp):
        cut = slice(t * width, (t + 1) * width)
        out[:, cut] = (members[t] * stretch * gain_two[:, cut]).astype(bf16)

    for k in range(1, n_sp):
        for grp in range(2):

            @pl.when(group_of(flip(sp, k)) == grp)
            def _():
                for i in range(3):
                    qkv(grp, k, i).wait_send()

        head_send_of(k).wait_send()
    for i in range(2):
        to_partner(i).wait_send()
    over.wait_send()
    for k in range(1, n_tp):
        share_stats(k).wait_send()

    def sent(e):
        for k in range(1, n_sp):
            dispatch(e, k).wait_send()
            give_back(e, k).wait_send()
        for k in range(2):
            over_y(e, k).wait_send()
            across(e, 0, k).wait_send()
            across(e, 1, k).wait_send()
            to_core(e, k).wait_send()
            to_far(e, k).wait_send()

    each(sent)
    for i in range(3):
        final(i).wait_send()


def layer_rows(
    tokens, qn, kn, vn, qb, kb, vb, mix_lambda, head_gain, proj_n, proj_b, gain_one, gain_two,
    expert_ids, expert_gates, wg, wu, wd,
):
    n_sp, n_tp = lax.axis_size("sp"), lax.axis_size("tp")
    count, model_width = tokens.shape
    heads = vn.shape[1] // V
    width = model_width // n_tp
    experts, hidden = wg.shape[0], wg.shape[2]
    slots = min(3, experts)
    filled = n_sp * CAP
    places = n_sp * experts * CAP
    bf16, f32 = jnp.bfloat16, jnp.float32
    dma = pltpu.SemaphoreType.DMA
    far = pl.BlockSpec(memory_space=pltpu.HBM)
    near = pl.BlockSpec(memory_space=pltpu.VMEM)
    vmem = lambda *shape: pltpu.VMEM(shape, bf16)
    wide = lambda *shape: pltpu.VMEM(shape, f32)
    like = lambda array: pltpu.VMEM(array.shape, array.dtype)
    ids, gates = expert_ids.T, expert_gates.T
    one, two = gain_one[None, :], gain_two[None, :]
    operands = (
        mix_lambda, ids, gates, tokens, qn, kn, vn, qb, kb, vb, head_gain, proj_n, proj_b,
        one, two, wg, wu, wd,
    )
    return pl.pallas_call(
        functools.partial(layer_kernel, n_sp, n_tp, heads),
        out_shape=pltpu.VMEM(tokens.shape, bf16),
        in_specs=[far] * len(operands),
        out_specs=near,
        scratch_shapes=[
            like(mix_lambda),
            like(ids),
            like(gates),
            vmem(count, width),
            like(qn),
            like(kn),
            like(vn),
            like(qb),
            like(kb),
            like(vb),
            like(head_gain),
            like(proj_n),
            like(proj_b),
            wide(1, width),
            like(two),
            vmem(slots, *wg.shape[1:]),
            vmem(slots, *wu.shape[1:]),
            vmem(slots, *wd.shape[1:]),
            vmem(n_sp * count, 2 * V),
            vmem(n_sp * count, 2 * V),
            vmem(n_sp * count, V),
            vmem(n_sp * count, V),
            vmem(count, 2 * heads * V),
            wide(count, model_width),
            vmem(2, count, width),
            vmem(2, count, width),
            vmem(count, width),
            vmem(count, width),
            wide(8, count),
            wide(n_tp, 8, count),
            vmem(count, width),
            vmem(places, count),
            vmem(count, places),
            vmem(experts, n_sp, CAP, width),
            vmem(n_tp, experts, n_sp, CAP, width),
            vmem(filled, hidden),
            vmem(n_tp, experts, filled, width),
            vmem(2, experts, filled, width),
            vmem(experts, filled, width),
            vmem(experts, n_sp, CAP, width),
            vmem(experts, n_sp, CAP, width),
            vmem(n_tp, count, width),
            dma((15,)),
            dma((3, slots)),
            dma((3, n_sp)),
            dma((3, n_sp)),
            dma((n_sp,)),
            dma((n_sp,)),
        ]
        + [dma((2,))] * 2
        + [dma((1,))] * 2
        + [dma((n_tp,))] * 2
        + [dma((experts, n_sp))] * 2
        + [dma((experts, 2))] * 2
        + [dma((experts, 4))] * 2
        + [dma((experts, 2))] * 4
        + [dma((experts, n_sp))] * 2
        + [dma((3,))] * 2,
        compiler_params=pltpu.CompilerParams(
            collective_id=0, has_side_effects=True, vmem_limit_bytes=61 * 2**20
        ),
        name="layer",
    )(*operands)


def head_fold(running, queries, key_rows, values, key_width):
    maxima, totals, weighted = running
    length = key_rows.shape[0]
    head_count = queries.shape[1]
    keyed = key_rows.reshape(length, head_count, 2, key_width)
    valued = values.reshape(length, head_count, V)
    scores = jnp.einsum(
        "qhmd,khmd->hmqk", queries, keyed, preferred_element_type=jnp.float32
    ) * key_width ** (-0.5)
    updated = jnp.maximum(maxima, jnp.max(scores, -1))
    exponent = jnp.exp(scores - updated[..., None])
    totals = jnp.sum(exponent, -1)
    weighted = jnp.einsum(
        "hmqk,khv->hmqv", exponent.astype(jnp.bfloat16), valued, preferred_element_type=jnp.float32
    )
    return (updated, totals, weighted)


def head_output(running, mixing, gains):
    maxima, totals, weighted = running
    diff = (
        weighted[:, 0] / totals[:, 0, :, None]
        - mixing[:, None, None] * weighted[:, 1] / totals[:, 1, :, None]
    )
    normed = (diff * lax.rsqrt(jnp.mean(diff * diff, -1, keepdims=True) + norm_eps) * gains).astype(
        jnp.bfloat16
    )
    return jnp.moveaxis(normed, 0, 1).reshape(normed.shape[1], -1)


def attention_gathered(
    tokens,
    query_narrow,
    key_narrow,
    value_narrow,
    query_broad,
    key_broad,
    value_broad,
    mix_lambda,
    head_gain,
    proj_narrow,
    proj_broad,
    gain_one,
):
    token_count = tokens.shape[0]
    head_count = value_narrow.shape[1] // V
    queries_first = query_narrow.reshape(token_count, head_count, 2, QK_NARROW)
    queries_second = query_broad.reshape(token_count, head_count, 2, QK_BROAD)
    start_state = (
        jnp.full((head_count, 2, token_count), -1e30, jnp.float32),
        jnp.zeros((head_count, 2, token_count), jnp.float32),
        jnp.zeros((head_count, 2, token_count, V), jnp.float32),
    )
    state_first = head_fold(
        start_state,
        queries_first,
        lax.all_gather(key_narrow, "sp", axis=0, tiled=True),
        lax.all_gather(value_narrow, "sp", axis=0, tiled=True),
        QK_NARROW,
    )
    state_second = head_fold(
        start_state,
        queries_second,
        lax.all_gather(key_broad, "sp", axis=0, tiled=True),
        lax.all_gather(value_broad, "sp", axis=0, tiled=True),
        QK_BROAD,
    )
    heads_first = head_output(state_first, mix_lambda[0], head_gain[0])
    heads_second = head_output(state_second, mix_lambda[1], head_gain[1])
    partial_value = jnp.dot(heads_first, proj_narrow, preferred_element_type=jnp.float32)
    partial_value = partial_value + jnp.dot(
        heads_second, proj_broad, preferred_element_type=jnp.float32
    )
    attn = lax.psum(
        partial_value.astype(jnp.bfloat16).astype(jnp.float32).astype(jnp.bfloat16), "tp"
    ).astype(jnp.float32)
    return layer_scale(deep_alpha * tokens.astype(jnp.float32) + attn, gain_one).astype(
        jnp.bfloat16
    )


def on_device(
    tokens,
    query_narrow,
    key_narrow,
    value_narrow,
    query_broad,
    key_broad,
    value_broad,
    mix_lambda,
    head_gain,
    proj_narrow,
    proj_broad,
    gain_one,
    gain_two,
    expert_ids,
    expert_gates,
    gate_weight,
    up_weight,
    down_weight,
):
    token_count = tokens.shape[0]
    model_width = tokens.shape[1]
    members = (
        tokens,
        query_narrow,
        key_narrow,
        value_narrow,
        query_broad,
        key_broad,
        value_broad,
        mix_lambda,
        head_gain,
        proj_narrow,
        proj_broad,
        gain_one,
    )
    n_sp, n_tp = lax.axis_size("sp"), lax.axis_size("tp")
    whole_heads = 2 * (value_narrow.shape[1] // V) == n_sp
    if whole_heads and n_tp // 2 == 2 and not n_sp & (n_sp - 1):
        return layer_rows(
            *members, gain_two, expert_ids, expert_gates, gate_weight, up_weight, down_weight
        )
    mixed_rows = attention_gathered(*members)
    experts_all = gate_weight.shape[0] * lax.axis_size("sp")
    chosen = expert_ids.reshape(-1)
    onehot = (chosen[:, None] == jnp.arange(experts_all, dtype=jnp.int32)[None, :]).astype(
        jnp.int32
    )
    before = jnp.cumsum(onehot, axis=0, dtype=jnp.int32) - onehot
    slot_index = jnp.sum(before * onehot, axis=-1, dtype=jnp.int32)
    position = (chosen * CAP + slot_index).reshape(expert_ids.shape)
    match = position[:, :, None] == jnp.arange(CAP * experts_all, dtype=jnp.int32)
    spread = jnp.any(match, axis=1).astype(jnp.bfloat16).T
    shares = jnp.sum(jnp.where(match, expert_gates[:, :, None], 0.0), axis=1)
    high = lax.reduce_precision(shares, 8, 7)
    low = (shares - high).astype(jnp.bfloat16)
    return expert_rows(
        mixed_rows,
        spread,
        high.astype(jnp.bfloat16),
        low,
        gain_two,
        gate_weight,
        up_weight,
        down_weight,
    )


def solution(mesh):
    return jax.shard_map(
        on_device,
        mesh=mesh,
        in_specs=(
            P("sp", None),
            P("sp", "tp"),
            P("sp", "tp"),
            P("sp", "tp"),
            P("sp", "tp"),
            P("sp", "tp"),
            P("sp", "tp"),
            P(None, "tp"),
            P(),
            P("tp", None),
            P("tp", None),
            P(),
            P(),
            P("sp", None),
            P("sp", None),
            P("sp", None, "tp"),
            P("sp", None, "tp"),
            P("sp", "tp", None),
        ),
        out_specs=P("sp", None),
        check_vma=False,
    )
```

```python
import functools

import jax
import jax.numpy as jnp
from jax import lax
from jax.experimental import pallas as pl
from jax.experimental.pallas import tpu as pltpu
from jax.sharding import PartitionSpec as P

QK_NARROW = 64
QK_BROAD = 128
V = 128
TOP = 2
CAP = 16


deep_alpha = 8.0**0.25
norm_eps = 1e-05


def layer_scale(inputs, gains):
    center = jnp.mean(inputs, -1, keepdims=True)
    spread = jnp.mean(jnp.square(inputs - center), -1, keepdims=True)
    return (inputs - center) * lax.rsqrt(spread + norm_eps) * gains


MESH = pl.DeviceIdType.MESH
LOG2E = 1.4426950408889634


def remote(src, dst, send, recv, axis, index):
    return pltpu.make_async_remote_copy(
        src_ref=src,
        dst_ref=dst,
        send_sem=send,
        recv_sem=recv,
        device_id={axis: index},
        device_id_type=MESH,
    )


def greet(n_sp, n_tp, sp, tp):
    barrier = pltpu.get_barrier_semaphore()
    for k in range(1, n_sp):
        pl.semaphore_signal(
            barrier, inc=1, device_id={"sp": lax.rem(sp + k, n_sp)}, device_id_type=MESH
        )
    for k in range(1, n_tp):
        pl.semaphore_signal(
            barrier, inc=1, device_id={"tp": lax.rem(tp + k, n_tp)}, device_id_type=MESH
        )
    pl.semaphore_wait(barrier, n_sp + n_tp - 2)


def lanes(index, width):
    return pl.ds(pl.multiple_of(index * width, width), width)


def expert_kernel(
    n_sp, n_tp, mixed, spread, high, low, gain_two, wg, wu, wd, out,
    gate, up, down, rows_out, rows_in, act, part, part_core, part_far, summed, back, routed,
    loaded, a_send, a_recv, y_send, y_recv, c_send, c_recv,
    d_send, d_recv, s_send, s_recv, b_send, b_recv, g_send, g_recv,
):
    sp, tp = lax.axis_index("sp"), lax.axis_index("tp")
    experts, slots, width = rows_out.shape[1:]
    hidden = act.shape[1]
    filled = n_sp * slots
    pairs = n_tp // 2
    y, c = tp // 2, tp % 2
    other = 2 * y + 1 - c

    def load(e, go):
        for i, (a, b) in enumerate(((wg, gate), (wu, up), (wd, down))):
            copy = pltpu.make_async_copy(a.at[e], b.at[e], loaded.at[i, e])
            copy.start() if go else copy.wait()

    def each(body):
        lax.fori_loop(0, experts, lambda e, _: (body(e), 0)[1], 0)

    each(lambda e: load(e, True))
    greet(n_sp, n_tp, sp, tp)

    mine = lanes(tp, width)
    picked = jnp.dot(spread[...], mixed[:, mine], preferred_element_type=jnp.float32)
    rows_out[...] = picked.astype(jnp.bfloat16).reshape(rows_out.shape)

    def dispatch(e, k):
        to = lax.rem(sp + k, n_sp)
        return remote(
            rows_out.at[to, e], rows_in.at[tp, e, sp], a_send.at[e, k], a_recv.at[e, k], "sp", to
        )

    def send_rows(e):
        for k in range(1, n_sp):
            dispatch(e, k).start()
        rows_in[tp, e, sp] = rows_out[sp, e]

    each(send_rows)

    def far(e, k):
        block = rows_in.at[tp, e]
        to = 2 * lax.rem(y + k, pairs) + c
        return remote(block, block, y_send.at[e, k], y_recv.at[e, k], "tp", to)

    def far_slot(k):
        return 2 * lax.rem(y + pairs - k, pairs) + c

    def across(e, k):
        block = rows_in.at[far_slot(k), e]
        return remote(block, block, c_send.at[e, k], c_recv.at[e, k], "tp", other)

    def pass_on(e):
        for k in range(1, n_sp):
            source = lax.rem(sp + n_sp - k, n_sp)
            block = rows_in.at[tp, e, source]
            remote(block, block, a_send.at[e, k], a_recv.at[e, k], "sp", source).wait_recv()
        for k in range(1, pairs):
            far(e, k).start()
        across(e, 0).start()

    each(pass_on)

    def pass_across(e):
        for k in range(1, pairs):
            block = rows_in.at[far_slot(k), e]
            remote(block, block, y_send.at[e, k], y_recv.at[e, k], "tp", far_slot(k)).wait_recv()
            across(e, k).start()

    def to_core(e, k):
        yy = lax.rem(y + k, pairs)
        return remote(
            part.at[2 * yy + 1 - c, e], part_core.at[k, e], d_send.at[e, k], d_recv.at[e, k],
            "tp", other,
        )

    def to_far(e, k):
        to = 2 * lax.rem(y + k, pairs) + c
        return remote(
            part.at[to, e], part_far.at[k, e], s_send.at[e, k], s_recv.at[e, k], "tp", to
        )

    def give_back(e, k):
        to = lax.rem(sp + k, n_sp)
        return remote(
            summed.at[e, to], back.at[sp, e], b_send.at[e, k], b_recv.at[e, k], "sp", to
        )

    tile = min(256, hidden)

    def compute(e):
        pass_across(e)
        load(e, False)
        for k in range(pairs):
            block = rows_in.at[2 * lax.rem(y + pairs - k, pairs) + 1 - c, e]
            remote(block, block, c_send.at[e, k], c_recv.at[e, k], "tp", other).wait_recv()
        inputs = jnp.concatenate(
            [rows_in[t, e].reshape(filled, width) for t in range(n_tp)], axis=1
        )

        def hidden_tile(j, _):
            cut = lanes(j, tile)
            gated = jnp.dot(inputs, gate[e, :, cut], preferred_element_type=jnp.float32)
            lifted = jnp.dot(inputs, up[e, :, cut], preferred_element_type=jnp.float32)
            act[:, cut] = (gated / (1.0 + jnp.exp(-gated)) * lifted).astype(jnp.bfloat16)
            return 0

        lax.fori_loop(0, hidden // tile, hidden_tile, 0)

        def down_tile(t, _):
            product = jnp.dot(
                act[...], down[e, :, lanes(t, width)], preferred_element_type=jnp.float32
            )
            part[t, e] = product.astype(jnp.bfloat16)
            return 0

        lax.fori_loop(0, n_tp, down_tile, 0)
        for k in range(pairs):
            to_core(e, k).start()

    def core_sum(e, k):
        block = part_core.at[k, e]
        remote(block, block, d_send.at[e, k], d_recv.at[e, k], "tp", other).wait_recv()
        slot = 2 * lax.rem(y + k, pairs) + c
        return part[slot, e].astype(jnp.float32) + part_core[k, e].astype(jnp.float32)

    def reduce_core(e):
        for k in range(1, pairs):
            total = core_sum(e, k)
            part[2 * lax.rem(y + k, pairs) + c, e] = total.astype(jnp.bfloat16)
            to_far(e, k).start()

    def reduce_far(e):
        total = core_sum(e, 0)
        for k in range(1, pairs):
            block = part_far.at[k, e]
            remote(block, block, s_send.at[e, k], s_recv.at[e, k], "tp", far_slot(k)).wait_recv()
            total = total + part_far[k, e].astype(jnp.float32)
        summed[e] = total.astype(jnp.bfloat16).reshape(n_sp, slots, width)
        for k in range(1, n_sp):
            give_back(e, k).start()
        back[sp, e] = summed[e, sp]

    def step(e, _):
        pl.when(e < experts)(lambda: compute(e))
        pl.when((e >= 1) & (e <= experts))(lambda: reduce_core(e - 1))
        pl.when(e >= 2)(lambda: reduce_far(e - 2))
        return 0

    lax.fori_loop(0, experts + 2, step, 0)

    def arrive(e):
        for k in range(1, n_sp):
            source = lax.rem(sp + n_sp - k, n_sp)
            block = back.at[source, e]
            remote(block, block, b_send.at[e, k], b_recv.at[e, k], "sp", source).wait_recv()

    each(arrive)
    returned = back[...].reshape(n_sp * experts * slots, width)
    weighted = jnp.dot(high[...], returned, preferred_element_type=jnp.float32) + jnp.dot(
        low[...], returned, preferred_element_type=jnp.float32
    )
    routed[:, mine] = weighted.astype(jnp.bfloat16)

    def share(k):
        to = lax.rem(tp + k, n_tp)
        block = routed.at[:, mine]
        return remote(block, block, g_send.at[k], g_recv.at[k], "tp", to)

    for k in range(1, n_tp):
        share(k).start()
    for k in range(1, n_tp):
        peer = lax.rem(tp + n_tp - k, n_tp)
        block = routed.at[:, lanes(peer, width)]
        remote(block, block, g_send.at[k], g_recv.at[k], "tp", peer).wait_recv()
    full = deep_alpha * mixed[...].astype(jnp.float32) + routed[...].astype(jnp.float32)
    out[...] = layer_scale(full, gain_two[...]).astype(jnp.bfloat16)

    def sent(e):
        for k in range(1, n_sp):
            dispatch(e, k).wait_send()
            give_back(e, k).wait_send()
        for k in range(pairs):
            across(e, k).wait_send()
            to_core(e, k).wait_send()
        for k in range(1, pairs):
            far(e, k).wait_send()
            to_far(e, k).wait_send()

    each(sent)
    for k in range(1, n_tp):
        share(k).wait_send()


def expert_rows(mixed, spread, high, low, gain_two, wg, wu, wd):
    n_sp, n_tp = lax.axis_size("sp"), lax.axis_size("tp")
    count, model_width = mixed.shape
    experts, hidden = wg.shape[0], wg.shape[2]
    width, pairs, filled = model_width // n_tp, n_tp // 2, n_sp * CAP
    bf16 = jnp.bfloat16
    dma = pltpu.SemaphoreType.DMA
    far = pl.BlockSpec(memory_space=pl.ANY)
    near = pl.BlockSpec(memory_space=pltpu.VMEM)
    vmem = lambda *shape: pltpu.VMEM(shape, bf16)
    return pl.pallas_call(
        functools.partial(expert_kernel, n_sp, n_tp),
        out_shape=jax.ShapeDtypeStruct(mixed.shape, bf16),
        in_specs=[near] * 5 + [far] * 3,
        out_specs=near,
        scratch_shapes=[
            vmem(*wg.shape),
            vmem(*wu.shape),
            vmem(*wd.shape),
            vmem(n_sp, experts, CAP, width),
            vmem(n_tp, experts, n_sp, CAP, width),
            vmem(filled, hidden),
            vmem(n_tp, experts, filled, width),
            vmem(pairs, experts, filled, width),
            vmem(pairs, experts, filled, width),
            vmem(experts, n_sp, CAP, width),
            vmem(n_sp, experts, CAP, width),
            vmem(count, model_width),
            dma((3, experts)),
        ]
        + [dma((experts, n_sp))] * 2
        + [dma((experts, pairs))] * 8
        + [dma((experts, n_sp))] * 2
        + [dma((n_tp,))] * 2,
        compiler_params=pltpu.CompilerParams(
            collective_id=1, has_side_effects=True, vmem_limit_bytes=67043328
        ),
        name="experts",
    )(mixed, spread, high, low, gain_two[None, :], wg, wu, wd)


def flip(index, mask):
    bit = 1
    while bit <= mask:
        if mask & bit:
            index = index + bit - 2 * bit * lax.rem(index // bit, 2)
        bit *= 2
    return index


def route(ids, gates, spread, shares, experts_all, owners):
    count = ids.shape[1]
    expert = lax.broadcasted_iota(jnp.int32, (experts_all, count), 0)
    picks = [(expert == ids[k : k + 1, :]).astype(jnp.float32) for k in range(TOP)]
    taken = functools.reduce(lambda a, b: a + b, picks)
    earlier = lax.broadcasted_iota(jnp.int32, (count, count), 0) < lax.broadcasted_iota(
        jnp.int32, (count, count), 1
    )
    before = jnp.dot(
        taken.astype(jnp.bfloat16),
        earlier.astype(jnp.float32).astype(jnp.bfloat16),
        preferred_element_type=jnp.float32,
    )
    place = lax.broadcasted_iota(jnp.int32, (experts_all * CAP, count), 0).astype(jnp.float32)
    weight = jnp.zeros((experts_all * CAP, count), jnp.float32)
    marked = jnp.zeros((experts_all * CAP, count), jnp.float32)
    for k in range(TOP):
        slot = jnp.sum(before * picks[k], 0, keepdims=True)
        chosen, own = ids[k : k + 1, :], experts_all // owners
        order = lax.rem(chosen, own) * owners + chosen // own
        position = order.astype(jnp.float32) * CAP + slot
        hit = place == position
        weight = weight + jnp.where(hit, gates[k : k + 1, :], 0.0)
        marked = marked + jnp.where(hit, 1.0, 0.0)
    spread[...] = marked.astype(jnp.bfloat16)
    shares[...] = weight.T.astype(jnp.bfloat16)


def layer_kernel(
    n_sp, n_tp, heads, lam_h, ids_h, gates_h, tok_h, qn_h, kn_h, vn_h, qb_h, kb_h, vb_h,
    gains_h, pn_h, pb_h, one_h, two_h, wg, wu, wd, out,
    lam, ids, gates, tok, qn, kn, vn, qb, kb, vb, gains, proj_n, proj_b, gain_one, gain_two,
    gate, up, down, q_all, k_all, v_all, head_out, head_in, early, pc_out, pc_in, py_out, py_in,
    st_out, st_in, mixed, spread, shares, rows_out, rows_in, act, part, part_core, part_far,
    summed, back, z_all,
    local, loaded, send, recv, head_send, head_recv, pc_send, pc_recv, py_send, py_recv,
    st_send, st_recv, a_send, a_recv, y_send, y_recv, c_send, c_recv, d_send, d_recv,
    s_send, s_recv, b_send, b_recv, g_send, g_recv,
):
    sp, tp = lax.axis_index("sp"), lax.axis_index("tp")
    y, c = tp // 2, lax.rem(tp, 2)
    core = 2 * y + 1 - c
    far = 2 * (1 - y) + c
    far_core = 2 * (1 - y) + 1 - c
    count, width = tok.shape
    lane = V
    bf16, f32 = jnp.bfloat16, jnp.float32
    experts, hidden = wg.shape[0], wg.shape[2]
    slots = gate.shape[0]
    filled = n_sp * CAP
    mine = lanes(tp, width)

    pairs = (
        (kn_h, kn), (vn_h, vn), (kb_h, kb), (vb_h, vb), (qn_h, qn), (qb_h, qb),
        (ids_h, ids), (gates_h, gates), (lam_h, lam), (gains_h, gains),
        (tok_h.at[:, mine], tok), (one_h.at[:, mine], gain_one), (two_h, gain_two),
        (pn_h, proj_n), (pb_h, proj_b),
    )
    copies = [pltpu.make_async_copy(a, b, local.at[i]) for i, (a, b) in enumerate(pairs)]
    for copy in copies:
        copy.start()

    def load(e, go):
        for i, (a, b) in enumerate(((wg, gate), (wu, up), (wd, down))):
            slot = lax.rem(e, slots)
            copy = pltpu.make_async_copy(a.at[e], b.at[slot], loaded.at[i, slot])
            copy.start() if go else copy.wait()

    def each(body):
        lax.fori_loop(0, experts, lambda e, _: (body(e), 0)[1], 0)

    lax.fori_loop(0, slots, lambda e, _: (load(e, True), 0)[1], 0)
    greet(n_sp, n_tp, sp, tp)

    def group_of(s):
        return lax.rem(s + s // 2, 2)

    def block_rows(s):
        return pl.ds(pl.multiple_of(s * count, count), count)

    rows = block_rows(sp)

    def piece(grp, head, i):
        size = lane * (1 if i == 2 else grp + 1)
        source = ((qn, kn, vn), (qb, kb, vb))[grp][i]
        return source.at[:, lanes(head, size)]

    def landing(grp, s, i):
        if i == 2:
            return v_all.at[block_rows(s)]
        return (q_all, k_all)[i].at[block_rows(s), 0 : lane * (grp + 1)]

    def qkv(grp, k, i):
        to = flip(sp, k)
        return remote(
            piece(grp, to // 2, i), landing(grp, sp, i), send.at[i, k], recv.at[i, k], "sp", to
        )

    def arrived(grp, k, i):
        source = flip(sp, k)
        block = landing(grp, source, i)
        remote(block, block, send.at[i, k], recv.at[i, k], "sp", source).wait_recv()

    my_group, my_head = group_of(sp), sp // 2

    near = n_sp // 2
    order = [*range(near - 1, 0, -1), *range(n_sp - 1, near - 1, -1)]

    def side_order(g):
        return order[near - 1 :] if g else order[: near - 1]

    def send_all(parts):
        for k in order:
            for grp in range(2):

                @pl.when(group_of(flip(sp, k)) == grp)
                def _():
                    for i in parts:
                        qkv(grp, k, i).start()

    for copy in copies[:4]:
        copy.wait()
    send_all((1, 2))
    for copy in copies[4:6]:
        copy.wait()
    send_all((0,))
    for grp in range(2):

        @pl.when(my_group == grp)
        def _():
            for i in range(3):
                landing(grp, sp, i)[...] = piece(grp, my_head, i)[...]

    for copy in copies[6:13]:
        copy.wait()
    route(ids, gates, spread, shares, n_sp * experts, n_sp)

    for grp in range(2):

        @pl.when(my_group == grp)
        def _():
            for k in range(1, n_sp):
                arrived(grp, k, 1)
                arrived(grp, k, 2)

    factor = jnp.where(my_group == 0, QK_NARROW**-0.5, QK_BROAD**-0.5) * LOG2E
    lam_row = lam[pl.ds(my_group, 1), :]
    mixing = jnp.sum(
        jnp.where(lax.broadcasted_iota(jnp.int32, lam_row.shape, 1) == my_head, lam_row, 0.0),
        -1,
        keepdims=True,
    )
    gain = gains[pl.ds(my_group, 1), :]
    col = my_group * heads + my_head

    def head_send_of(k):
        s = flip(sp, k)
        return remote(
            head_out.at[block_rows(s), :], head_in.at[:, lanes(col, lane)],
            head_send.at[k], head_recv.at[k], "sp", s,
        )

    def attend(ks):
        for grp in range(2):

            @pl.when(my_group == grp)
            def _():
                for k in ks:
                    if k:
                        arrived(grp, k, 0)

        span = len(ks) * count
        first = flip(sp, ks[0]) // len(ks)
        q_rows = pl.ds(pl.multiple_of(first * span, span), span)
        keep_all = jnp.broadcast_to(my_group, (span, lane)) == 1
        place = lax.broadcasted_iota(jnp.int32, (span, lane), 1) // QK_NARROW
        parts = []
        for m in range(2):
            cut = lanes(my_group * m, lane)
            queries = q_all[q_rows, cut].astype(f32)
            queries = jnp.where(keep_all | (place == m), queries, 0.0).astype(bf16)
            scores = lax.dot_general(
                queries, k_all[:, cut], (((1,), (1,)), ((), ())), preferred_element_type=f32
            )
            highest = jnp.max(scores, -1, keepdims=True)
            expo = jnp.exp2((scores - highest) * factor)
            total = jnp.sum(expo, -1, keepdims=True)
            numer = jnp.dot(expo.astype(bf16), v_all[...], preferred_element_type=f32)
            parts.append(numer / total)
        diff = parts[0] - mixing * parts[1]
        normed = diff * lax.rsqrt(jnp.mean(diff * diff, -1, keepdims=True) + norm_eps) * gain
        head_out[q_rows, :] = normed.astype(bf16)
        for k in ks[::-1]:
            if k:
                head_send_of(k).start()
            else:
                head_in[:, lanes(col, lane)] = head_out[rows, :]

    for k in (*range(0, near, 2), *range(n_sp - 2, near - 1, -2)):
        attend((k, k + 1))

    for copy in copies[13:]:
        copy.wait()

    def head_arrived(k):
        s = flip(sp, k)
        target = head_in.at[:, lanes(group_of(s) * heads + s // 2, lane)]
        remote(target, target, head_send.at[k], head_recv.at[k], "sp", s).wait_recv()

    side = heads * lane // 2
    half = sp // (n_sp // 2)

    def projected(which, cut):
        at = pl.ds(pl.multiple_of(which * side, side), side)
        wide = pl.ds(pl.multiple_of(which * side + 2 * side, side), side)
        return jnp.dot(head_in[:, at], proj_n[at, cut], preferred_element_type=f32) + jnp.dot(
            head_in[:, wide], proj_b[at, cut], preferred_element_type=f32
        )

    for k in range(1, n_sp // 2):
        head_arrived(k)
    for t in range(n_tp):
        cut = slice(t * width, (t + 1) * width)
        early[:, cut] = projected(half, cut)
    for k in range(n_sp // 2, n_sp):
        head_arrived(k)

    def quarter(t):
        cut = lanes(t, width)
        return early[:, cut] + projected(1 - half, cut)

    def to_partner(i):
        return remote(pc_out.at[i], pc_in.at[i], pc_send.at[i], pc_recv.at[i], "tp", core)

    def partner(i):
        remote(pc_in.at[i], pc_in.at[i], pc_send.at[i], pc_recv.at[i], "tp", core).wait_recv()
        return pc_in[i].astype(f32)

    over = remote(py_out, py_in, py_send.at[0], py_recv.at[0], "tp", far)
    pc_out[0] = quarter(far_core).astype(bf16)
    to_partner(0).start()
    product = quarter(far)
    pc_out[1] = quarter(core).astype(bf16)
    to_partner(1).start()
    py_out[...] = (product + partner(0)).astype(bf16)
    over.start()
    summed_own = quarter(tp) + partner(1) + deep_alpha * tok[...].astype(f32)
    over.wait_recv()
    full = summed_own + py_in[...].astype(f32)

    center = jnp.mean(full, -1, keepdims=True)
    apart = full - center
    squares = jnp.sum(apart * apart, -1, keepdims=True)
    which = lax.broadcasted_iota(jnp.int32, (count, lane), 1)
    st_out[...] = jnp.where(which == 0, center, squares).T[: st_out.shape[0]]

    def share_stats(k):
        to = lax.rem(tp + k, n_tp)
        return remote(st_out, st_in.at[k], st_send.at[k], st_recv.at[k], "tp", to)

    for k in range(1, n_tp):
        share_stats(k).start()
    st_in[0] = st_out[...]
    for k in range(1, n_tp):
        share_stats(k).wait_recv()
    means = [st_in[k, 0:1, :] for k in range(n_tp)]
    mean = sum(means[1:], means[0]) / n_tp
    spreads = [
        st_in[k, 1:2, :] + width * jnp.square(means[k] - mean) for k in range(n_tp)
    ]
    scale = lax.rsqrt(sum(spreads[1:], spreads[0]) / (n_tp * width) + norm_eps)
    upright = jnp.where(
        lax.broadcasted_iota(jnp.int32, (lane, count), 0) == 0, mean, scale
    ).T
    mixed[...] = ((full - upright[:, 0:1]) * upright[:, 1:2] * gain_one[...]).astype(bf16)


    def dispatch(e, k):
        to = flip(sp, k)
        return remote(
            rows_out.at[e, to], rows_in.at[tp, e, sp], a_send.at[e, k], a_recv.at[e, k], "sp", to
        )

    def send_rows(e):
        at = pl.ds(pl.multiple_of(e * filled, filled), filled)
        picked = jnp.dot(spread[at, :], mixed[...], preferred_element_type=f32)
        rows_out[e] = picked.astype(bf16).reshape(rows_out.shape[1:])
        for k in order:
            dispatch(e, k).start()
        rows_in[tp, e, sp] = rows_out[e, sp]

    each(send_rows)

    def side_of(g):
        return pl.ds(pl.multiple_of((half if g == 0 else 1 - half) * near, near), near)

    def over_y(e, g):
        block = rows_in.at[tp, e, side_of(g)]
        return remote(block, block, y_send.at[e, g], y_recv.at[e, g], "tp", far)

    def across(e, k, g):
        block = rows_in.at[(tp, far)[k], e, side_of(g)]
        i = 2 * k + g
        return remote(block, block, c_send.at[e, i], c_recv.at[e, i], "tp", core)

    def pass_on(e, g):
        for k in side_order(g):
            source = flip(sp, k)
            block = rows_in.at[tp, e, source]
            remote(block, block, a_send.at[e, k], a_recv.at[e, k], "sp", source).wait_recv()
        over_y(e, g).start()
        across(e, 0, g).start()

    def pass_across(e, g):
        block = rows_in.at[far, e, side_of(g)]
        remote(block, block, y_send.at[e, g], y_recv.at[e, g], "tp", far).wait_recv()
        across(e, 1, g).start()

    def ready(e):
        for k, t in enumerate((core, far_core)):
            for g in range(2):
                block = rows_in.at[t, e, side_of(g)]
                i = 2 * k + g
                remote(block, block, c_send.at[e, i], c_recv.at[e, i], "tp", core).wait_recv()

    def to_core(e, k):
        t = (core, far_core)[k]
        return remote(
            part.at[t, e], part_core.at[k, e], d_send.at[e, k], d_recv.at[e, k], "tp", core
        )

    def rows_for(g):
        size = near * CAP
        return pl.ds(pl.multiple_of((half if g == 0 else 1 - half) * size, size), size)

    def to_far(e, g):
        at = rows_for(g)
        return remote(
            part.at[far, e, at], part_far.at[e, at], s_send.at[e, g], s_recv.at[e, g], "tp", far
        )

    def give_back(e, k):
        to = flip(sp, k)
        return remote(
            summed.at[e, to], back.at[e, sp], b_send.at[e, k], b_recv.at[e, k], "sp", to
        )

    def core_arrived(e, k):
        block = part_core.at[k, e]
        remote(block, block, d_send.at[e, k], d_recv.at[e, k], "tp", core).wait_recv()

    def reduce_core(e, g):
        if g == 1:
            core_arrived(e, 1)
        at = rows_for(g)
        total = part[far, e, at].astype(f32) + part_core[1, e, at].astype(f32)
        part[far, e, at] = total.astype(bf16)
        to_far(e, g).start()

    def reduce_far(e, g):
        if g == 1:
            core_arrived(e, 0)
        at = rows_for(g)
        block = part_far.at[e, at]
        remote(block, block, s_send.at[e, g], s_recv.at[e, g], "tp", far).wait_recv()
        total = part[tp, e, at].astype(f32) + part_core[0, e, at].astype(f32)
        total = total + part_far[e, at].astype(f32)
        summed[e, side_of(g)] = total.astype(bf16).reshape(near, CAP, width)
        for k in side_order(g):
            give_back(e, k).start()
        if g == 0:
            back[e, sp] = summed[e, sp]

    tile = min(512, hidden)

    def compute(e, _):
        slot = lax.rem(e, slots)
        load(e, False)
        ready(e)
        inputs = jnp.concatenate(
            [rows_in[t, e].reshape(filled, width) for t in range(n_tp)], axis=1
        )

        for j in range(hidden // tile):
            cut = slice(j * tile, (j + 1) * tile)
            gated = jnp.dot(inputs, gate[slot, :, cut], preferred_element_type=f32)
            lifted = jnp.dot(inputs, up[slot, :, cut], preferred_element_type=f32)
            act[:, cut] = (gated / (1.0 + jnp.exp(-gated)) * lifted).astype(bf16)
        pl.when(e + 2 < experts)(lambda: pass_on(e + 2, 1))
        pl.when(e + 3 < experts)(lambda: pass_on(e + 3, 0))

        @pl.when(e + 1 < experts)
        def _():
            pass_across(e + 1, 0)
            pl.when(e + 2 < experts)(lambda: pass_across(e + 1, 1))

        pl.when(e >= 2)(lambda: reduce_far(e - 2, 1))
        pl.when(e >= 1)(lambda: reduce_core(e - 1, 0))
        pl.when(e >= 3)(lambda: reduce_far(e - 3, 0))

        for i, t in enumerate((far_core, far, core, tp)):
            product = jnp.dot(
                act[...], down[slot, :, lanes(t, width)], preferred_element_type=f32
            )
            part[t, e] = product.astype(bf16)
            if i in (0, 2):
                to_core(e, 1 - i // 2).start()
        pl.when(e + slots < experts)(lambda: load(e + slots, True))
        reduce_core(e, 1)
        pl.when(e + 2 == experts)(lambda: pass_across(e + 1, 1))
        return 0

    pass_on(0, 0)
    if experts > 1:
        pass_on(1, 0)
    pass_on(0, 1)
    pass_across(0, 0)
    if experts > 1:
        pass_on(1, 1)
    if experts > 2:
        pass_on(2, 0)
    pass_across(0, 1)
    lax.fori_loop(0, experts, compute, 0)
    last = range(max(0, experts - 2), experts)
    reduce_core(experts - 1, 0)
    for e in last:
        reduce_far(e, 1)
        if e + 1 < experts and experts > 2:
            reduce_far(experts - 3, 0)
    for e in last:
        reduce_far(e, 0)

    def arrive(e, total):
        for k in order:
            source = flip(sp, k)
            block = back.at[e, source]
            remote(block, block, b_send.at[e, k], b_recv.at[e, k], "sp", source).wait_recv()
        at = slice(e * filled, (e + 1) * filled)
        return total + jnp.dot(
            shares[:, at], back[e].reshape(filled, width), preferred_element_type=f32
        )

    total = deep_alpha * mixed[...].astype(f32)
    for e in range(experts):
        total = arrive(e, total)
    z_all[tp] = total.astype(bf16)

    def final(i):
        t, to = ((tp, far), (tp, core), (far, core))[i]
        return remote(z_all.at[t], z_all.at[t], g_send.at[i], g_recv.at[i], "tp", to)

    def final_wait(i):
        t, source = ((far, far), (core, core), (far_core, core))[i]
        remote(z_all.at[t], z_all.at[t], g_send.at[i], g_recv.at[i], "tp", source).wait_recv()

    final(0).start()
    final(1).start()
    final_wait(0)
    final(2).start()
    final_wait(1)
    final_wait(2)
    members = [z_all[t].astype(f32) for t in range(n_tp)]
    sums = [jnp.sum(z, -1, keepdims=True) for z in members]
    middle = sum(sums[1:], sums[0]) / (n_tp * width)
    members = [z - middle for z in members]
    sums = [jnp.sum(z * z, -1, keepdims=True) for z in members]
    stretch = lax.rsqrt(sum(sums[1:], sums[0]) / (n_tp * width) + norm_eps)
    for t in range(n_tp):
        cut = slice(t * width, (t + 1) * width)
        out[:, cut] = (members[t] * stretch * gain_two[:, cut]).astype(bf16)

    for k in range(1, n_sp):
        for grp in range(2):

            @pl.when(group_of(flip(sp, k)) == grp)
            def _():
                for i in range(3):
                    qkv(grp, k, i).wait_send()

        head_send_of(k).wait_send()
    for i in range(2):
        to_partner(i).wait_send()
    over.wait_send()
    for k in range(1, n_tp):
        share_stats(k).wait_send()

    def sent(e):
        for k in range(1, n_sp):
            dispatch(e, k).wait_send()
            give_back(e, k).wait_send()
        for k in range(2):
            over_y(e, k).wait_send()
            across(e, 0, k).wait_send()
            across(e, 1, k).wait_send()
            to_core(e, k).wait_send()
            to_far(e, k).wait_send()

    each(sent)
    for i in range(3):
        final(i).wait_send()


def layer_rows(
    tokens, qn, kn, vn, qb, kb, vb, mix_lambda, head_gain, proj_n, proj_b, gain_one, gain_two,
    expert_ids, expert_gates, wg, wu, wd,
):
    n_sp, n_tp = lax.axis_size("sp"), lax.axis_size("tp")
    count, model_width = tokens.shape
    heads = vn.shape[1] // V
    width = model_width // n_tp
    experts, hidden = wg.shape[0], wg.shape[2]
    slots = min(3, experts)
    filled = n_sp * CAP
    places = n_sp * experts * CAP
    bf16, f32 = jnp.bfloat16, jnp.float32
    dma = pltpu.SemaphoreType.DMA
    far = pl.BlockSpec(memory_space=pltpu.HBM)
    near = pl.BlockSpec(memory_space=pltpu.VMEM)
    vmem = lambda *shape: pltpu.VMEM(shape, bf16)
    wide = lambda *shape: pltpu.VMEM(shape, f32)
    like = lambda array: pltpu.VMEM(array.shape, array.dtype)
    ids, gates = expert_ids.T, expert_gates.T
    one, two = gain_one[None, :], gain_two[None, :]
    operands = (
        mix_lambda, ids, gates, tokens, qn, kn, vn, qb, kb, vb, head_gain, proj_n, proj_b,
        one, two, wg, wu, wd,
    )
    return pl.pallas_call(
        functools.partial(layer_kernel, n_sp, n_tp, heads),
        out_shape=pltpu.VMEM(tokens.shape, bf16),
        in_specs=[far] * len(operands),
        out_specs=near,
        scratch_shapes=[
            like(mix_lambda),
            like(ids),
            like(gates),
            vmem(count, width),
            like(qn),
            like(kn),
            like(vn),
            like(qb),
            like(kb),
            like(vb),
            like(head_gain),
            like(proj_n),
            like(proj_b),
            wide(1, width),
            like(two),
            vmem(slots, *wg.shape[1:]),
            vmem(slots, *wu.shape[1:]),
            vmem(slots, *wd.shape[1:]),
            vmem(n_sp * count, 2 * V),
            vmem(n_sp * count, 2 * V),
            vmem(n_sp * count, V),
            vmem(n_sp * count, V),
            vmem(count, 2 * heads * V),
            wide(count, model_width),
            vmem(2, count, width),
            vmem(2, count, width),
            vmem(count, width),
            vmem(count, width),
            wide(8, count),
            wide(n_tp, 8, count),
            vmem(count, width),
            vmem(places, count),
            vmem(count, places),
            vmem(experts, n_sp, CAP, width),
            vmem(n_tp, experts, n_sp, CAP, width),
            vmem(filled, hidden),
            vmem(n_tp, experts, filled, width),
            vmem(2, experts, filled, width),
            vmem(experts, filled, width),
            vmem(experts, n_sp, CAP, width),
            vmem(experts, n_sp, CAP, width),
            vmem(n_tp, count, width),
            dma((15,)),
            dma((3, slots)),
            dma((3, n_sp)),
            dma((3, n_sp)),
            dma((n_sp,)),
            dma((n_sp,)),
        ]
        + [dma((2,))] * 2
        + [dma((1,))] * 2
        + [dma((n_tp,))] * 2
        + [dma((experts, n_sp))] * 2
        + [dma((experts, 2))] * 2
        + [dma((experts, 4))] * 2
        + [dma((experts, 2))] * 4
        + [dma((experts, n_sp))] * 2
        + [dma((3,))] * 2,
        compiler_params=pltpu.CompilerParams(
            collective_id=0, has_side_effects=True, vmem_limit_bytes=61 * 2**20
        ),
        name="layer",
    )(*operands)


def head_fold(running, queries, key_rows, values, key_width):
    maxima, totals, weighted = running
    length = key_rows.shape[0]
    head_count = queries.shape[1]
    keyed = key_rows.reshape(length, head_count, 2, key_width)
    valued = values.reshape(length, head_count, V)
    scores = jnp.einsum(
        "qhmd,khmd->hmqk", queries, keyed, preferred_element_type=jnp.float32
    ) * key_width ** (-0.5)
    updated = jnp.maximum(maxima, jnp.max(scores, -1))
    exponent = jnp.exp(scores - updated[..., None])
    totals = jnp.sum(exponent, -1)
    weighted = jnp.einsum(
        "hmqk,khv->hmqv", exponent.astype(jnp.bfloat16), valued, preferred_element_type=jnp.float32
    )
    return (updated, totals, weighted)


def head_output(running, mixing, gains):
    maxima, totals, weighted = running
    diff = (
        weighted[:, 0] / totals[:, 0, :, None]
        - mixing[:, None, None] * weighted[:, 1] / totals[:, 1, :, None]
    )
    normed = (diff * lax.rsqrt(jnp.mean(diff * diff, -1, keepdims=True) + norm_eps) * gains).astype(
        jnp.bfloat16
    )
    return jnp.moveaxis(normed, 0, 1).reshape(normed.shape[1], -1)


def attention_gathered(
    tokens,
    query_narrow,
    key_narrow,
    value_narrow,
    query_broad,
    key_broad,
    value_broad,
    mix_lambda,
    head_gain,
    proj_narrow,
    proj_broad,
    gain_one,
):
    token_count = tokens.shape[0]
    head_count = value_narrow.shape[1] // V
    queries_first = query_narrow.reshape(token_count, head_count, 2, QK_NARROW)
    queries_second = query_broad.reshape(token_count, head_count, 2, QK_BROAD)
    start_state = (
        jnp.full((head_count, 2, token_count), -1e30, jnp.float32),
        jnp.zeros((head_count, 2, token_count), jnp.float32),
        jnp.zeros((head_count, 2, token_count, V), jnp.float32),
    )
    state_first = head_fold(
        start_state,
        queries_first,
        lax.all_gather(key_narrow, "sp", axis=0, tiled=True),
        lax.all_gather(value_narrow, "sp", axis=0, tiled=True),
        QK_NARROW,
    )
    state_second = head_fold(
        start_state,
        queries_second,
        lax.all_gather(key_broad, "sp", axis=0, tiled=True),
        lax.all_gather(value_broad, "sp", axis=0, tiled=True),
        QK_BROAD,
    )
    heads_first = head_output(state_first, mix_lambda[0], head_gain[0])
    heads_second = head_output(state_second, mix_lambda[1], head_gain[1])
    partial_value = jnp.dot(heads_first, proj_narrow, preferred_element_type=jnp.float32)
    partial_value = partial_value + jnp.dot(
        heads_second, proj_broad, preferred_element_type=jnp.float32
    )
    attn = lax.psum(
        partial_value.astype(jnp.bfloat16).astype(jnp.float32).astype(jnp.bfloat16), "tp"
    ).astype(jnp.float32)
    return layer_scale(deep_alpha * tokens.astype(jnp.float32) + attn, gain_one).astype(
        jnp.bfloat16
    )


def on_device(
    tokens,
    query_narrow,
    key_narrow,
    value_narrow,
    query_broad,
    key_broad,
    value_broad,
    mix_lambda,
    head_gain,
    proj_narrow,
    proj_broad,
    gain_one,
    gain_two,
    expert_ids,
    expert_gates,
    gate_weight,
    up_weight,
    down_weight,
):
    token_count = tokens.shape[0]
    model_width = tokens.shape[1]
    members = (
        tokens,
        query_narrow,
        key_narrow,
        value_narrow,
        query_broad,
        key_broad,
        value_broad,
        mix_lambda,
        head_gain,
        proj_narrow,
        proj_broad,
        gain_one,
    )
    n_sp, n_tp = lax.axis_size("sp"), lax.axis_size("tp")
    whole_heads = 2 * (value_narrow.shape[1] // V) == n_sp
    if whole_heads and n_tp // 2 == 2 and not n_sp & (n_sp - 1):
        return layer_rows(
            *members, gain_two, expert_ids, expert_gates, gate_weight, up_weight, down_weight
        )
    mixed_rows = attention_gathered(*members)
    experts_all = gate_weight.shape[0] * lax.axis_size("sp")
    chosen = expert_ids.reshape(-1)
    onehot = (chosen[:, None] == jnp.arange(experts_all, dtype=jnp.int32)[None, :]).astype(
        jnp.int32
    )
    before = jnp.cumsum(onehot, axis=0, dtype=jnp.int32) - onehot
    slot_index = jnp.sum(before * onehot, axis=-1, dtype=jnp.int32)
    position = (chosen * CAP + slot_index).reshape(expert_ids.shape)
    match = position[:, :, None] == jnp.arange(CAP * experts_all, dtype=jnp.int32)
    spread = jnp.any(match, axis=1).astype(jnp.bfloat16).T
    shares = jnp.sum(jnp.where(match, expert_gates[:, :, None], 0.0), axis=1)
    high = lax.reduce_precision(shares, 8, 7)
    low = (shares - high).astype(jnp.bfloat16)
    return expert_rows(
        mixed_rows,
        spread,
        high.astype(jnp.bfloat16),
        low,
        gain_two,
        gate_weight,
        up_weight,
        down_weight,
    )


def solution(mesh):
    return jax.shard_map(
        on_device,
        mesh=mesh,
        in_specs=(
            P("sp", None),
            P("sp", "tp"),
            P("sp", "tp"),
            P("sp", "tp"),
            P("sp", "tp"),
            P("sp", "tp"),
            P("sp", "tp"),
            P(None, "tp"),
            P(),
            P("tp", None),
            P("tp", None),
            P(),
            P(),
            P("sp", None),
            P("sp", None),
            P("sp", None, "tp"),
            P("sp", None, "tp"),
            P("sp", "tp", None),
        ),
        out_specs=P("sp", None),
        check_vma=False,
    )
```
